32 devices in a mesh: ep: 8 (over z, core), tp: 4 (over y, x).
Axes of the slice: x: 2, y: 2, z: 4, core: 2. Of those that a mesh axis runs over, the one named last changes fastest.
Arguments:
- queries: bfloat16 [2048, 2048], P('ep', 'tp'), may hold values from -6 to 6
- keys: bfloat16 [2048, 2048], P('ep', 'tp'), may hold values from -6 to 6
- values: bfloat16 [2048, 2048], P('ep', 'tp'), may hold values from -6 to 6
- gates: bfloat16 [2048, 2048], P('ep', 'tp'), may hold values from -6 to 6
- log_decay: float32 [2048, 16], P('ep', 'tp'), may hold values from -2 to 0
- out_weight: bfloat16 [2048, 2048], P(None, 'tp'), may hold values from -0.125 to 0.125
- moe_rows: bfloat16 [2048, 2048], P('ep'), may hold values from -140 to 140
- moe_gain: bfloat16 [2048], replicated, may hold values from 0.099609375 to 1.8984375
- routes: int32 [2048, 2], P('ep'), may hold values from 0 to 7, as said below
- route_weights: float32 [2048, 2], P('ep'), may hold values from 0.1 to 1
- gate_proj: bfloat16 [8, 2048, 4096], P('ep', None, 'tp'), may hold values from -0.125 to 0.125
- up_proj: bfloat16 [8, 2048, 4096], P('ep', None, 'tp'), may hold values from -0.125 to 0.125
- down_proj: bfloat16 [8, 4096, 2048], P('ep', None, 'tp'), may hold values from -0.09375 to 0.09375
Outputs:
- mixer_out: bfloat16 [2048, 2048], P('ep', 'tp')
- moe_out: bfloat16 [2048, 2048], P('ep', 'tp')
The draws below stay inside these ranges and needn't reach their ends.
Inputs may be any that keep to these rules, and one draw needn't show every extreme that they name: `routes`: each row names two different experts of one group of 8 consecutive experts; in each aligned block of 256 rows every expert is named by exactly 64 rows.
All inputs are finite; a program needn't handle non-finite values.
Results may differ from the reference program's by a relative error of at most 0.011.
Values may be sent and summed in bfloat16 or wider, within the bound.
A program may use at most 64 MiB of HBM per device.

```python
import math
import jax
import jax.numpy as jnp
from jax import lax

D = 2048
RETENTION_HEADS = 16
HEAD_DIM = 128
FF = 4096
EXP_GROUP = 8
BLOCK = 128
ROWS_MIX = 256
ROWS_MOE = 256
MIXER_TOKENS = 2048
TOKENS_MOE = 2048
EXPERTS = 8
GROUPS = 1


def draw_log_decay(key, part):
    k_fast = jax.random.fold_in(key, 11)
    k_rate = jax.random.fold_in(key, 12)
    k_slow = jax.random.fold_in(key, 13)
    k_block = jax.random.fold_in(key, 14)
    k_rough = jax.random.fold_in(key, 15)
    location_random_key = jax.random.fold_in(key, 16)
    spike_random_key = jax.random.fold_in(key, 17)
    fast_share = 0.5
    is_fast = jax.random.uniform(k_fast, (RETENTION_HEADS,)) < fast_share
    fast_rate = jax.random.uniform(k_rate, (RETENTION_HEADS,), minval=2.5, maxval=4.0) / BLOCK
    slow_rate = jax.random.uniform(k_slow, (RETENTION_HEADS,), minval=0.1, maxval=0.35) / MIXER_TOKENS
    baseline_decay_rate = jnp.where(is_fast, fast_rate, slow_rate)
    span_count = MIXER_TOKENS // ROWS_MIX
    extent_multiplier = jnp.exp(jax.random.uniform(k_block, (span_count, RETENTION_HEADS), minval=-math.log(2.0), maxval=math.log(2.0)))
    extent_multiplier = jnp.repeat(extent_multiplier, ROWS_MIX, axis=0)
    jitter_multiplier = jnp.exp(jax.random.uniform(k_rough, (MIXER_TOKENS, RETENTION_HEADS), minval=-0.7, maxval=0.7))
    spike_locations = jax.random.randint(location_random_key, (2, RETENTION_HEADS), 0, MIXER_TOKENS)
    spike_strength = jnp.log(jax.random.uniform(spike_random_key, (2, RETENTION_HEADS), minval=0.5, maxval=0.8))
    token_place = jnp.arange(MIXER_TOKENS, dtype=jnp.int32)[None, :, None]
    decay_spikes = jnp.sum(jnp.where(token_place == spike_locations[:, None, :], spike_strength[:, None, :], 0.0), axis=0)
    return (decay_spikes - baseline_decay_rate[None, :] * extent_multiplier * jitter_multiplier).astype(jnp.float32)


def draw_moe_rows(key, part):
    k_base = jax.random.fold_in(key, 21)
    k_column = jax.random.fold_in(key, 22)
    base = jax.random.truncated_normal(k_base, -4.0, 4.0, (TOKENS_MOE, D))
    column_scale = jnp.exp(jax.random.uniform(k_column, (D,), minval=0.0, maxval=math.log(10.0)))
    result = base * column_scale[None, :]
    return result.astype(jnp.bfloat16)


def draw_routes(key, part):
    k_perm = jax.random.fold_in(key, 31)
    k_first = jax.random.fold_in(key, 32)
    k_second = jax.random.fold_in(key, 33)
    span_count = TOKENS_MOE // ROWS_MOE
    orders = jax.vmap(lambda single: jax.random.permutation(single, ROWS_MOE))(jax.random.split(k_perm, span_count))
    ranked = jnp.argsort(orders, axis=1, stable=True).astype(jnp.int32)
    group_id = ranked % GROUPS
    local_rank = ranked // GROUPS
    first_offset = jax.random.randint(k_first, (span_count, GROUPS), 0, EXP_GROUP)
    second_offset = jax.random.randint(k_second, (span_count, GROUPS), 0, EXP_GROUP - 1)
    first_pick = (local_rank + jnp.take_along_axis(first_offset, group_id, axis=1)) % EXP_GROUP
    second_step = (local_rank // EXP_GROUP + jnp.take_along_axis(second_offset, group_id, axis=1)) % (EXP_GROUP - 1)
    second_pick = (first_pick + 1 + second_step) % EXP_GROUP
    chosen = jnp.stack([group_id * EXP_GROUP + first_pick, group_id * EXP_GROUP + second_pick], axis=-1)
    return chosen.reshape(TOKENS_MOE, 2).astype(jnp.int32)


def block_levels(stream_key, dims, cuts, least, high):
    def one(dim, shards_of):
        draws = jax.random.uniform(jax.random.fold_in(jax.random.fold_in(stream_key, 6), dim), (shards_of,), jnp.float32, least / len(cuts), high / len(cuts))
        return jnp.repeat(jnp.exp(draws), dims[dim] // shards_of).reshape((-1,) + (1,) * (len(dims) - dim - 1))

    gain = one(*cuts[0])
    for cut in cuts[1:]:
        gain = gain * one(*cut)
    return gain


def centred(own_key, extent, scale, limit, cuts=(), kind=jnp.bfloat16):
    level = block_levels(own_key, extent, cuts, -0.22, 0.18) if cuts else 1.0
    drawn = jax.random.normal(own_key, extent, jnp.float32) * scale * level
    return jnp.minimum(jnp.maximum(drawn, -limit), limit).astype(kind)


def setup_inputs(seed: int = 0) -> dict:
    arg_keys = jax.random.split(jax.random.key(seed), 14)
    queries = centred(arg_keys[0], (MIXER_TOKENS, RETENTION_HEADS * HEAD_DIM), 1.0, 6.0, ((0, 8), (1, 4)))
    keys = centred(arg_keys[1], (MIXER_TOKENS, RETENTION_HEADS * HEAD_DIM), 1.0, 6.0, ((0, 8), (1, 4)))
    values = centred(arg_keys[2], (MIXER_TOKENS, RETENTION_HEADS * HEAD_DIM), 1.0, 6.0, ((0, 8), (1, 4)))
    gates = centred(arg_keys[3], (MIXER_TOKENS, RETENTION_HEADS * HEAD_DIM), 1.0, 6.0, ((0, 8), (1, 4)))
    log_decay = draw_log_decay(jax.random.fold_in(arg_keys[13], 71), 0)
    out_weight = centred(arg_keys[5], (RETENTION_HEADS * HEAD_DIM, D), (RETENTION_HEADS * HEAD_DIM) ** -0.5, 0.125, ((1, 4),))
    moe_rows = draw_moe_rows(jax.random.fold_in(arg_keys[13], 71), 0)
    moe_gain = jnp.clip(1.0 + 0.18 * jax.random.normal(arg_keys[7], (D,), jnp.float32), 0.099609375, 1.8984375).astype(jnp.bfloat16)
    routes = draw_routes(jax.random.fold_in(arg_keys[13], 71), 0)
    route_weights = jnp.clip(0.1 + 0.9 * jax.random.uniform(arg_keys[9], (TOKENS_MOE, 2), jnp.float32) ** block_levels(arg_keys[9], (TOKENS_MOE, 2), ((0, 8),), -0.2, 0.2), 0.1, 1.0)
    gate_proj = centred(arg_keys[10], (EXPERTS, D, FF), D ** -0.5, 0.125, ((0, 8), (2, 4)))
    up_proj = centred(arg_keys[11], (EXPERTS, D, FF), D ** -0.5, 0.125, ((0, 8), (2, 4)))
    down_proj = centred(arg_keys[12], (EXPERTS, FF, D), FF ** -0.5, 0.09375, ((0, 8), (2, 4)))
    return {"queries": queries, "keys": keys, "values": values, "gates": gates, "log_decay": log_decay, "out_weight": out_weight, "moe_rows": moe_rows, "moe_gain": moe_gain, "routes": routes, "route_weights": route_weights, "gate_proj": gate_proj, "up_proj": up_proj, "down_proj": down_proj}


def rotate(source, factor):
    length = source.shape[0]
    values_f = source.astype(jnp.float32).reshape(length, RETENTION_HEADS, HEAD_DIM)
    half_dim = HEAD_DIM // 2
    inverse = 10000.0 ** (-jnp.arange(half_dim, dtype=jnp.float32) / half_dim)
    angles = jnp.arange(length, dtype=jnp.float32)[:, None] * inverse[None, :]
    cosine = jnp.cos(angles)[:, None, :]
    sine_part = jnp.sin(angles)[:, None, :]
    first_half = values_f[..., :half_dim]
    second_half = values_f[..., half_dim:]
    turned = jnp.concatenate([first_half * cosine - second_half * sine_part, first_half * sine_part + second_half * cosine], axis=-1)
    return (turned * factor).astype(jnp.bfloat16)

def retention_ref(queries, keys, values, gates, log_decay, out_weight):
    length = queries.shape[0]
    block_count = length // BLOCK
    rot_q = rotate(queries, 1.0)
    rot_k = rotate(keys, HEAD_DIM ** (-0.5))
    q_blocks = rot_q.reshape(block_count, BLOCK, RETENTION_HEADS, HEAD_DIM)
    k_blocks = rot_k.reshape(block_count, BLOCK, RETENTION_HEADS, HEAD_DIM)
    v_blocks = values.reshape(block_count, BLOCK, RETENTION_HEADS, HEAD_DIM)
    l_blocks = log_decay.reshape(block_count, BLOCK, RETENTION_HEADS)
    causal = jnp.arange(BLOCK)[:, None] >= jnp.arange(BLOCK)[None, :]

    def advance(carry_state, member):
        q_block, k_block, v_block, l_block = member
        cumulative = jnp.cumsum(l_block, axis=0)
        across = cumulative.T
        spread = across[:, :, None] - across[:, None, :]
        weights = jnp.where(causal, jnp.exp(jnp.where(causal, spread, 0.0)), 0.0)
        q_float = q_block.astype(jnp.float32)
        k_float = k_block.astype(jnp.float32)
        v_float = v_block.astype(jnp.float32)
        scores = jnp.einsum('ihd,jhd->hij', q_float, k_float)
        rounded = lax.optimization_barrier((scores * weights).astype(jnp.bfloat16)).astype(jnp.float32)
        inside = jnp.einsum('hij,jhd->ihd', rounded, v_float)
        carried = jnp.einsum('ihd,hde->ihe', q_float, carry_state, precision=lax.Precision.HIGHEST) * jnp.exp(cumulative)[:, :, None]
        ending = cumulative[-1]
        k_scaled = k_float * jnp.exp(ending[None, :] - cumulative)[:, :, None]
        update = jnp.einsum('jhd,jhe->hde', k_scaled, v_float, precision=lax.Precision.HIGHEST)
        return (jnp.exp(ending)[:, None, None] * carry_state + update, inside + carried)
    zero_state = jnp.zeros((RETENTION_HEADS, HEAD_DIM, HEAD_DIM), jnp.float32)
    _, retained = lax.scan(advance, zero_state, (q_blocks, k_blocks, v_blocks, l_blocks))
    retained = retained.reshape(length, RETENTION_HEADS, HEAD_DIM)
    gate_f = gates.astype(jnp.float32).reshape(length, RETENTION_HEADS, HEAD_DIM)
    scaled = retained * lax.rsqrt(lax.optimization_barrier(jnp.mean(retained * retained, axis=-1, keepdims=True)) + 1e-05)
    head_out = (scaled * jax.nn.silu(gate_f)).astype(jnp.bfloat16).reshape(length, RETENTION_HEADS * HEAD_DIM)
    return jnp.dot(head_out, out_weight, preferred_element_type=jnp.float32).astype(jnp.bfloat16)

def experts_ref(moe_rows, moe_gain, routes, route_weights, gate_proj, up_proj, down_proj):
    as_float = moe_rows.astype(jnp.float32)
    normed = (as_float * lax.rsqrt(lax.optimization_barrier(jnp.mean(as_float * as_float, axis=-1, keepdims=True)) + 1e-06) * moe_gain.astype(jnp.float32)).astype(jnp.bfloat16)
    flat_ids = routes.reshape(-1)
    sorted_slots = jnp.argsort(flat_ids, stable=True).astype(jnp.int32)
    per_expert = flat_ids.shape[0] // EXPERTS
    grouped = normed[sorted_slots // 2].reshape(EXPERTS, per_expert, D)

    def run_expert(member):
        block_rows, w_gate, w_up, w_down = member
        gate_part = jnp.dot(block_rows, w_gate, preferred_element_type=jnp.float32)
        up_part = jnp.dot(block_rows, w_up, preferred_element_type=jnp.float32)
        hidden = (jax.nn.silu(gate_part) * up_part).astype(jnp.bfloat16)
        return jnp.dot(hidden, w_down, preferred_element_type=jnp.float32).astype(jnp.bfloat16)
    outputs = lax.map(run_expert, (grouped, gate_proj, up_proj, down_proj))
    slot_out = jnp.zeros((flat_ids.shape[0], D), jnp.bfloat16).at[sorted_slots].set(outputs.reshape(-1, D))
    weighted = slot_out.astype(jnp.float32).reshape(-1, 2, D) * route_weights[:, :, None]
    return lax.optimization_barrier(jnp.sum(weighted, axis=1)).astype(jnp.bfloat16)

def reference(queries, keys, values, gates, log_decay, out_weight, moe_rows, moe_gain, routes, route_weights, gate_proj, up_proj, down_proj):
    mixer_out = retention_ref(queries, keys, values, gates, log_decay, out_weight)
    moe_out = experts_ref(moe_rows, moe_gain, routes, route_weights, gate_proj, up_proj, down_proj)
    return (mixer_out, moe_out)
```

```python
import functools

import jax
import jax.numpy as jnp
import numpy as np
from jax import lax
from jax.experimental import pallas as pl
from jax.experimental.pallas import tpu as pltpu
from jax.sharding import PartitionSpec as P

BLOCK = 128
MESH = pl.DeviceIdType.MESH
F32 = jnp.float32
BF16 = jnp.bfloat16


def each(low, high, body):
    if high - low <= 8:
        for index in range(low, high):
            body(index)
    else:

        @pl.loop(low, high)
        def _(index):
            body(index)


def span(index, size):
    return pl.ds(pl.multiple_of(index * size, size), size)


def split(value):
    high = value.astype(BF16)
    return high, (value - high.astype(F32)).astype(BF16)


def dot(a, b, dims=((1,), (0,))):
    return lax.dot_general(a, b, (dims, ((), ())), preferred_element_type=F32)


def chunk_units(ep):
    g = ep // 4
    return [(0, g), (2 * g, g), (g, g), (3 * g, g // 2), (3 * g + g // 2, g // 2)]


class Gather:
    def __init__(self, tp, region, half, send, recv):
        self.tp, self.region, self.half, self.send, self.recv = tp, region, half, send, recv
        self.me = lax.axis_index("tp")

    def copy(self, ref, slot, to):
        return pltpu.make_async_remote_copy(
            src_ref=ref, dst_ref=ref, send_sem=self.send(slot), recv_sem=self.recv(slot),
            device_id={"tp": to}, device_id_type=MESH,
        )

    def outs(self):
        me, tp = self.me, self.tp
        if tp == 4:
            return [self.copy(self.region(me), k - 1, me ^ k) for k in (1, 2)]
        return [self.copy(self.region(me), k - 1, lax.rem(me + k, tp)) for k in range(1, tp)]

    def hops(self):
        me = self.me
        return [
            self.copy(self.half(me ^ 1, 0), 2, me ^ 2),
            self.copy(self.half(me ^ 2, 1), 3, me ^ 1),
        ]

    def start(self):
        for copy in self.outs():
            copy.start()

    def forward(self):
        if self.tp == 4:
            me = self.me
            hops = self.hops()
            for k in (1, 2):
                self.copy(self.region(me ^ k), k - 1, me ^ k).wait_recv()
                hops[k - 1].start()

    def finish(self):
        me, tp = self.me, self.tp
        if tp == 4:
            self.copy(self.half(me ^ 3, 0), 2, me ^ 2).wait_recv()
            self.copy(self.half(me ^ 3, 1), 3, me ^ 1).wait_recv()
        else:
            for k in range(1, tp):
                owner = lax.rem(me + tp - k, tp)
                self.copy(self.region(owner), k - 1, owner).wait_recv()

    def drain(self):
        for copy in self.outs() + (self.hops() if self.tp == 4 else []):
            copy.wait_send()


def kernel(
    ep, tp,
    q_hbm, k_hbm, v_hbm, g_hbm, ld_ref, tab_hbm, rows_hbm, gain_ref, routes_ref, rw_ref,
    wo_hbm, wg_hbm, wu_hbm, wd_hbm,
    mix_hbm, moe_hbm,
    q_ref, k_ref, v_ref, g_ref, tab, rows_ref, turn,
    wo, wg, wu, wd, normed, p0, p1, og, x, h, eo, ret, ho, state, landed, excl,
    rq, inside, cums, pack, narrow, mix_out, moe_out,
    w_sem, z_send, z_recv, f_send, f_recv, h_send, h_recv, r_send, r_recv, m_send, m_recv,
    s_send, s_recv, o_sem,
):

    e, t = lax.axis_index("ep"), lax.axis_index("tp")
    rows, d = rows_ref.shape
    cap = 2 * rows // ep
    dq = d // tp
    ff = wd.shape[0]
    fq = ff // tp
    heads = ld_ref.shape[0]
    hd = q_ref.shape[1] // heads
    blocks = rows // BLOCK
    g = ep // 4
    units = chunk_units(ep)
    tile = min(256, fq)
    pieces = 2 if fq >= 512 else 1
    piece = fq // pieces
    core, chip, chips = lax.rem(e, 2), e // 2, ep // 2

    barrier = pltpu.get_barrier_semaphore()

    def greet_ep(off):
        pl.semaphore_signal(barrier, inc=1, device_id={"ep": e ^ off}, device_id_type=MESH)

    each(1, ep, greet_ep)
    for k in range(1, tp):
        pl.semaphore_signal(
            barrier, inc=1, device_id={"tp": lax.rem(t + k, tp)}, device_id_type=MESH
        )

    parts = 2
    step_rows = rows // parts
    part_at = [slice(i * step_rows, (i + 1) * step_rows) for i in range(parts)]
    row_loads = [
        pltpu.make_async_copy(rows_hbm.at[at, :], rows_ref.at[at, :], w_sem.at[7 + i])
        for i, at in enumerate(part_at)
    ]
    loads = [
        pltpu.make_async_copy(src, dst, w_sem.at[i])
        for i, (src, dst) in enumerate(
            (
                (wd_hbm.at[0], wd), (wo_hbm, wo),
                (q_hbm, q_ref), (k_hbm, k_ref), (v_hbm, v_ref), (g_hbm, g_ref), (tab_hbm, tab),
            )
        )
    ]
    weight_loads = [
        [
            pltpu.make_async_copy(
                src.at[0, :, j * piece : (j + 1) * piece], dst.at[:, j * piece : (j + 1) * piece],
                w_sem.at[9 + 2 * j + i],
            )
            for i, (src, dst) in enumerate(((wg_hbm, wg), (wu_hbm, wu)))
        ]
        for j in range(pieces)
    ]
    for load in row_loads + sum(weight_loads, []):
        load.start()

    routes = [routes_ref[k : k + 1, :] for k in range(2)]
    experts = lax.broadcasted_iota(jnp.int32, (max(8, ep), rows), 0)
    hot = [(experts == routes[k]).astype(F32) for k in range(2)]
    before = (
        lax.broadcasted_iota(jnp.int32, (rows, rows), 0)
        < lax.broadcasted_iota(jnp.int32, (rows, rows), 1)
    ).astype(F32).astype(BF16)
    rank = dot((hot[0] + hot[1]).astype(BF16), before)
    targets = [
        routes[k] * cap + jnp.sum(rank * hot[k], axis=0, keepdims=True).astype(jnp.int32)
        for k in range(2)
    ]

    for i, at in enumerate(part_at):
        row_loads[i].wait()
        squares = None
        for c in range(d // 128):
            val = rows_ref[at, c * 128 : (c + 1) * 128].astype(F32)
            squares = val * val if squares is None else squares + val * val
        scale = lax.rsqrt(jnp.sum(squares, axis=-1, keepdims=True) / d + 1e-06)
        for c in range(d // 128):
            cols = slice(c * 128, (c + 1) * 128)
            val = rows_ref[at, cols].astype(F32)
            normed[at, cols] = (val * scale * gain_ref[c : c + 1, :].astype(F32)).astype(BF16)

    def unit_at(low, size):
        return span((e // size) ^ (low // size), size * cap)

    def pick(low, size):
        slot = lax.broadcasted_iota(jnp.int32, (size * cap, rows), 0) + (
            (e // size) ^ (low // size)
        ) * (size * cap)
        return ((slot == targets[0]) | (slot == targets[1])).astype(F32).astype(BF16)

    def group(low, size, start, width):
        chosen = pick(low, size)
        wide = min(256, width)
        for c in range(width // wide):
            cols = pl.ds(pl.multiple_of(start + c * wide, wide), wide)
            og[unit_at(low, size), cols] = dot(chosen, normed[:, cols]).astype(BF16)

    group(0, g, 0, d)
    group(2 * g, g, t * dq, dq)
    pl.semaphore_wait(barrier, ep - 1 + tp - 1)

    def z_copy(off, here, whole):
        other = e ^ off
        land = span(other if here else e, cap)
        if whole:
            src, dst = og.at[span(other, cap), :], x.at[land, :]
        else:
            src, dst = og.at[span(other, cap), span(t, dq)], x.at[land, span(t, dq)]
        return pltpu.make_async_remote_copy(
            src_ref=src, dst_ref=dst, send_sem=z_send.at[other],
            recv_sem=z_recv.at[other if here else e],
            device_id={"ep": other}, device_id_type=MESH,
        )

    slim = [(2, g), (2 * g, 3 * g)]
    full = [(g, 2 * g), (3 * g, 4 * g)]

    def z_start(low, high, whole):
        each(low, high, lambda off: z_copy(off, False, whole).start())

    z_start(1, 2, True)
    for low, high in slim:
        z_start(low, high, False)
    for load in loads[2:7] + loads[0:2]:
        load.start()
    x[span(e, cap), :] = og[span(e, cap), :]
    for low, high in full:
        group(low, high - low, 0, d)

    @pl.when(core == 0)
    def _():
        z_start(*full[0], True)


    def row_gather(off):
        other = e ^ off
        start = other * cap

        def half(owner, k):
            return x.at[
                pl.ds(pl.multiple_of(start + k * (cap // 2), cap // 2), cap // 2), span(owner, dq)
            ]

        return Gather(
            tp, lambda owner: x.at[span(other, cap), span(owner, dq)], half,
            lambda slot: f_send.at[other, slot], lambda slot: f_recv.at[other, slot],
        )

    def hid_gather(u, j):
        low, size = units[u]
        count = size * cap
        base = ((e // size) ^ (low // size)) * count

        def cols(owner):
            return pl.ds(pl.multiple_of(owner * fq + j * piece, piece), piece)

        return Gather(
            tp,
            lambda owner: h.at[pl.ds(pl.multiple_of(base, count), count), cols(owner)],
            lambda owner, k: h.at[
                pl.ds(pl.multiple_of(base + k * (count // 2), count // 2), count // 2), cols(owner)
            ],
            lambda slot: h_send.at[u * pieces + j, slot],
            lambda slot: h_recv.at[u * pieces + j, slot],
        )

    half_rows = rows // 2

    def mix_gather(b):
        def at(low, size):
            return slice(b * half_rows + low, b * half_rows + low + size)

        return Gather(
            tp, lambda owner: ho.at[at(0, half_rows), span(owner, heads * hd)],
            lambda owner, k: ho.at[
                at(k * (half_rows // 2), half_rows // 2), span(owner, heads * hd)
            ],
            lambda slot: m_send.at[b, slot], lambda slot: m_recv.at[b, slot],
        )

    def take_rows(off):
        z_copy(off, True, False).wait_recv()
        row_gather(off).start()

    def hidden_piece(u, j):
        at = unit_at(*units[u])

        @pl.loop(0, piece // tile)
        def _(i):
            cols = pl.ds(pl.multiple_of(j * piece + i * tile, tile), tile)
            held = x[at, :]
            gate = dot(held, wg[:, cols])
            up = dot(held, wu[:, cols])
            hid = (gate / (1.0 + jnp.exp(-gate)) * up).astype(BF16)
            h[at, pl.ds(pl.multiple_of(t * fq + j * piece + i * tile, tile), tile)] = hid

        hid_gather(u, j).start()

    def back_copy(off, here):
        other = e ^ off
        return pltpu.make_async_remote_copy(
            src_ref=eo.at[span(other, cap), :], dst_ref=ret.at[span(other if here else e, cap), :],
            send_sem=r_send.at[other], recv_sem=r_recv.at[other if here else e],
            device_id={"ep": other}, device_id_type=MESH,
        )

    out_tile = min(256, dq)

    def down(u):
        for j in range(pieces):
            hid_gather(u, j).finish()
        low, size = units[u]
        at = unit_at(low, size)

        @pl.loop(0, dq // out_tile)
        def _(i):
            cols = pl.ds(pl.multiple_of(i * out_tile, out_tile), out_tile)
            eo[at, cols] = dot(h[at, :], wd[:, cols]).astype(BF16)

        each(max(1, low), low + size, lambda off: back_copy(off, False).start())
        if low == 0:
            ret[span(e, cap), :] = eo[span(e, cap), :]

    def forward(u, j):
        hid_gather(u, j).forward()

    row_i = lax.broadcasted_iota(jnp.int32, (BLOCK, BLOCK), 0)
    col_j = lax.broadcasted_iota(jnp.int32, (BLOCK, BLOCK), 1)
    causal = row_i >= col_j
    lower = causal.astype(F32)
    factor = hd ** (-0.5)
    decay_at = heads * hd

    def retention_local():
        pack[...] = jnp.zeros_like(pack)
        pack[0:1, :] = targets[0].astype(F32)
        pack[1:2, :] = targets[1].astype(F32)
        pack[2:4, :] = rw_ref[...]
        pack[4 : 4 + heads, :] = ld_ref[...]
        for b in range(rows // 128):
            narrow[b * 128 : (b + 1) * 128, :] = pack[:, b * 128 : (b + 1) * 128].T
        lanes = lax.broadcasted_iota(jnp.int32, (rows, ep * cap), 1)
        for k, ref in ((0, p0), (1, p1)):
            ref[...] = (lanes == narrow[:, k : k + 1].astype(jnp.int32)).astype(F32).astype(BF16)
        for load in loads[2:7]:
            load.wait()
        here_cos = tab[pl.ds(2 * rows + e, 1), :]
        here_sin = tab[pl.ds(2 * rows + ep + e, 1), :]
        sign = jnp.where(lax.broadcasted_iota(jnp.int32, (BLOCK, hd), 1) < hd // 2, -1.0, 1.0)
        for b in range(blocks):
            at = slice(b * BLOCK, (b + 1) * BLOCK)
            cos, sin = tab[at, :], tab[slice(rows + b * BLOCK, rows + (b + 1) * BLOCK), :]
            turn[0, at, :] = cos * here_cos - sin * here_sin
            turn[1, at, :] = (sin * here_cos + cos * here_sin) * sign
            cums[at, :] = lax.dot_general(
                lower, narrow[at, :], (((1,), (0,)), ((), ())),
                preferred_element_type=F32, precision=lax.Precision.HIGHEST,
            )
        for n in range(heads):
            cols = slice(n * hd, (n + 1) * hd)
            total = None
            gone = None
            for b in range(blocks):
                at = slice(b * BLOCK, (b + 1) * BLOCK)
                cos, sin = turn[0, at, :], turn[1, at, :]

                def turned(ref):
                    val = ref[at, cols].astype(F32)
                    return val * cos + pltpu.roll(val, hd // 2, 1) * sin

                qb = turned(q_ref).astype(BF16)
                kb = (turned(k_ref) * factor).astype(BF16)
                vb = v_ref[at, cols]
                rq[at, cols] = qb
                cum = jnp.broadcast_to(cums[at, 4 + n : 5 + n], (BLOCK, BLOCK))
                spread = cum - cum.T
                weight = jnp.where(causal, jnp.exp(jnp.where(causal, spread, 0.0)), 0.0)
                scores = dot(qb, kb, ((1,), (1,)))
                inside[at, cols] = dot((scores * weight).astype(BF16), vb)
                ending = cum[BLOCK - 1 : BLOCK, :]
                k_hi, k_lo = split(kb.astype(F32) * jnp.exp(ending - cum))
                update = dot(k_hi, vb, ((0,), (0,))) + dot(k_lo, vb, ((0,), (0,)))
                if b == 0:
                    total, gone = update, ending
                else:
                    total = jnp.exp(ending) * total + update
                    gone = gone + ending
                if b < blocks - 1:
                    excl[1 + b, n * hd : (n + 1) * hd, :] = total
            state[0, n * hd : (n + 1) * hd, :] = total
            state[0, decay_at + n : decay_at + n + 1, :] = jnp.exp(gone)
        excl[0, :decay_at, :] = jnp.zeros((decay_at, hd), F32)

    def up_copy():
        return pltpu.make_async_remote_copy(
            src_ref=state.at[0], dst_ref=landed.at[0], send_sem=s_send.at[0],
            recv_sem=s_recv.at[0], device_id={"ep": e ^ 1}, device_id_type=MESH,
        )

    def next_copy():
        return pltpu.make_async_remote_copy(
            src_ref=state.at[1, :decay_at, :], dst_ref=landed.at[1, :decay_at, :],
            send_sem=s_send.at[1], recv_sem=s_recv.at[1],
            device_id={"ep": lax.rem(e + 2, ep)}, device_id_type=MESH,
        )

    def down_copy():
        part = landed.at[1, :decay_at, :]
        return pltpu.make_async_remote_copy(
            src_ref=part, dst_ref=part, send_sem=s_send.at[2], recv_sem=s_recv.at[2],
            device_id={"ep": e ^ 1}, device_id_type=MESH,
        )

    def decays(n):
        at = slice(decay_at + n, decay_at + n + 1)
        return landed[0, at, :], state[0, at, :]

    def scan_open():
        @pl.when(core == 1)
        def _():
            up_copy().wait_recv()
            for n in range(heads):
                at = slice(n * hd, (n + 1) * hd)
                mine = decays(n)[1]
                state[1, at, :] = mine * landed[0, at, :] + state[0, at, :]
                excl[0, at, :] = landed[0, at, :]

        if chips > 1:

            @pl.when((core == 1) & (chip == 0))
            def _():
                next_copy().start()

    def scan_pass(turn_of):
        @pl.when((core == 1) & turn_of)
        def _():
            next_copy().wait_recv()
            down_copy().start()
            for n in range(heads):
                at = slice(n * hd, (n + 1) * hd)
                first, mine = decays(n)
                came = landed[1, at, :]
                state[1, at, :] = (first * mine) * came + state[1, at, :]
                excl[0, at, :] = first * came + excl[0, at, :]

        @pl.when((core == 1) & turn_of & (chip < chips - 1))
        def _():
            next_copy().start()

    def scan_close():
        @pl.when((core == 0) & (chip > 0))
        def _():
            down_copy().wait_recv()
            excl[0, :decay_at, :] = landed[1, :decay_at, :]

    def retention_close():
        for n in range(heads):
            cols = slice(n * hd, (n + 1) * hd)
            sat = slice(n * hd, (n + 1) * hd)
            entering = excl[0, sat, :]
            gone = None
            for b in range(blocks):
                at = slice(b * BLOCK, (b + 1) * BLOCK)
                cum = jnp.broadcast_to(cums[at, 4 + n : 5 + n], (BLOCK, hd))
                held = entering if b == 0 else jnp.exp(gone) * entering + excl[b, sat, :]
                hi, lo = split(held)
                qb = rq[at, cols]
                retained = inside[at, cols] + (dot(qb, hi) + dot(qb, lo)) * jnp.exp(cum)
                scale = lax.rsqrt(jnp.mean(retained * retained, axis=-1, keepdims=True) + 1e-05)
                gate = g_ref[at, cols].astype(F32)
                out = (retained * scale * (gate / (1.0 + jnp.exp(-gate)))).astype(BF16)
                ho[at, pl.ds(pl.multiple_of(t * heads * hd + n * hd, hd), hd)] = out
                ending = cum[BLOCK - 1 : BLOCK, :]
                gone = ending if gone is None else gone + ending

    for load in weight_loads[0]:
        load.wait()
    z_copy(1, True, True).wait_recv()
    each(2, g, take_rows)
    each(2, g, lambda off: row_gather(off).forward())
    each(2, g, lambda off: row_gather(off).finish())
    hidden_piece(0, 0)
    retention_local()

    @pl.when(core == 0)
    def _():
        up_copy().start()

    for j in range(1, pieces):
        for load in weight_loads[j]:
            load.wait()
        hidden_piece(0, j)
    scan_open()
    last = full[1][1] - (full[1][1] - full[1][0]) // 2

    @pl.when(core == 1)
    def _():
        z_start(*full[0], True)
        z_start(full[1][0], last, True)

    @pl.when(core == 0)
    def _():
        z_start(*full[1], True)


    each(2 * g, 3 * g, take_rows)
    each(2 * g, 3 * g, lambda off: row_gather(off).forward())
    for j in range(pieces):
        forward(0, j)
    scan_pass(chip == 1)

    @pl.when(core == 1)
    def _():
        z_start(last, full[1][1], True)

    each(2 * g, 3 * g, lambda off: row_gather(off).finish())
    for j in range(pieces):
        hidden_piece(1, j)

    each(g, 2 * g, lambda off: z_copy(off, True, True).wait_recv())
    for j in range(pieces):
        hidden_piece(2, j)
    loads[0].wait()
    down(0)
    forward(1, 0)
    scan_pass(chip == 2)
    for j in range(1, pieces):
        forward(1, j)
    forward(2, 0)

    def last_rows(u):
        low, size = units[u]
        each(low, low + size, lambda off: z_copy(off, True, True).wait_recv())
        for j in range(pieces):
            hidden_piece(u, j)

    last_rows(3)
    for j in range(1, pieces):
        forward(2, j)
    scan_pass(chip > 2)
    scan_close()
    retention_close()
    mix_gather(0).start()
    last_rows(4)
    down(1)
    for j in range(pieces):
        forward(3, j)
    down(2)
    mix_gather(0).forward()
    for j in range(pieces):
        forward(4, j)
    mix_gather(1).start()
    down(3)
    down(4)
    mix_gather(1).forward()
    loads[1].wait()

    for b in range(2):
        mix_gather(b).finish()

    @pl.loop(0, dq // out_tile)
    def _(i):
        cols = pl.ds(pl.multiple_of(i * out_tile, out_tile), out_tile)
        mix_out[:, cols] = dot(ho[...], wo[:, cols]).astype(BF16)

    mix_write = pltpu.make_async_copy(mix_out, mix_hbm, o_sem.at[0])
    mix_write.start()
    each(1, ep, lambda off: back_copy(off, True).wait_recv())

    @pl.loop(0, dq // out_tile)
    def _(i):
        cols = pl.ds(pl.multiple_of(i * out_tile, out_tile), out_tile)
        came = ret[:, cols]
        moe_out[:, cols] = (
            dot(p0[...], came) * narrow[:, 2:3] + dot(p1[...], came) * narrow[:, 3:4]
        ).astype(BF16)

    moe_write = pltpu.make_async_copy(moe_out, moe_hbm, o_sem.at[1])
    moe_write.start()

    def drain(low, high, whole):
        each(low, high, lambda off: z_copy(off, False, whole).wait_send())

    drain(1, 2, True)
    for low, high in slim:
        drain(low, high, False)
        each(low, high, lambda off: row_gather(off).drain())
    for low, high in full:
        drain(low, high, True)
    each(1, ep, lambda off: back_copy(off, False).wait_send())
    for u in range(len(units)):
        for j in range(pieces):
            hid_gather(u, j).drain()
    for b in range(2):
        mix_gather(b).drain()

    @pl.when(core == 0)
    def _():
        up_copy().wait_send()

    @pl.when((core == 1) & (chip < chips - 1))
    def _():
        next_copy().wait_send()

    @pl.when((core == 1) & (chip > 0))
    def _():
        down_copy().wait_send()

    mix_write.wait()
    moe_write.wait()


def turn_table(ep, rows, hd):
    half = hd // 2
    inverse = np.tile(10000.0 ** (-np.arange(half) / half), 2)
    near = np.arange(rows)[:, None] * inverse[None, :]
    far = (np.arange(ep) * rows)[:, None] * inverse[None, :]
    parts = [np.cos(near), np.sin(near), np.cos(far), np.sin(far)]
    return np.concatenate(parts).astype(np.float32)


def on_device(
    ep, tp,
    queries, keys, values, gates, log_decay, out_weight, moe_rows, moe_gain, routes,
    route_weights, gate_proj, up_proj, down_proj,
):
    rows, d = moe_rows.shape
    heads = log_decay.shape[1]
    width = queries.shape[1]
    hd = width // heads
    cap = 2 * rows // ep
    dq = d // tp
    fq = gate_proj.shape[2]
    ff = down_proj.shape[1]
    slots = max(4, tp - 1)
    pieces = len(chunk_units(ep)) * 2
    blocks = rows // BLOCK
    srows = heads * hd + 8 * ((heads + 7) // 8)
    vmem = pl.BlockSpec(memory_space=pltpu.VMEM)
    hbm = pl.BlockSpec(memory_space=pl.ANY)
    dma = pltpu.SemaphoreType.DMA
    out = jax.ShapeDtypeStruct((rows, dq), BF16)
    table = jnp.asarray(turn_table(ep, rows, hd))
    return pl.pallas_call(
        functools.partial(kernel, ep, tp),
        out_shape=(out, out),
        in_specs=[hbm] * 4 + [vmem, hbm, hbm] + [vmem] * 3 + [hbm] * 4,
        out_specs=(hbm, hbm),
        scratch_shapes=[
            pltpu.VMEM((rows, width), BF16),
            pltpu.VMEM((rows, width), BF16),
            pltpu.VMEM((rows, width), BF16),
            pltpu.VMEM((rows, width), BF16),
            pltpu.VMEM(table.shape, F32),
            pltpu.VMEM((rows, d), BF16),
            pltpu.VMEM((2, rows, hd), F32),
            pltpu.VMEM(out_weight.shape, BF16),
            pltpu.VMEM((d, fq), BF16),
            pltpu.VMEM((d, fq), BF16),
            pltpu.VMEM((ff, dq), BF16),
            pltpu.VMEM((rows, d), BF16),
            pltpu.VMEM((rows, ep * cap), BF16),
            pltpu.VMEM((rows, ep * cap), BF16),
            pltpu.VMEM((ep * cap, d), BF16),
            pltpu.VMEM((ep * cap, d), BF16),
            pltpu.VMEM((ep * cap, ff), BF16),
            pltpu.VMEM((ep * cap, dq), BF16),
            pltpu.VMEM((ep * cap, dq), BF16),
            pltpu.VMEM((rows, width * tp), BF16),
            pltpu.VMEM((2, srows, hd), F32),
            pltpu.VMEM((2, srows, hd), F32),
            pltpu.VMEM((blocks, srows, hd), F32),
            pltpu.VMEM((rows, width), BF16),
            pltpu.VMEM((rows, width), F32),
            pltpu.VMEM((rows, 128), F32),
            pltpu.VMEM((128, rows), F32),
            pltpu.VMEM((rows, 128), F32),
            pltpu.VMEM((rows, dq), BF16),
            pltpu.VMEM((rows, dq), BF16),
            dma((13,)),
            dma((ep,)), dma((ep,)),
            dma((ep, slots)), dma((ep, slots)),
            dma((pieces, slots)), dma((pieces, slots)),
            dma((ep,)), dma((ep,)),
            dma((2, slots)), dma((2, slots)),
            dma((3,)), dma((3,)),
            dma((2,)),
        ],
        compiler_params=pltpu.CompilerParams(
            collective_id=0, has_side_effects=True, vmem_limit_bytes=60 * 1024 * 1024
        ),
    )(
        queries, keys, values, gates, log_decay.T, table, moe_rows, moe_gain.reshape(-1, 128),
        routes.T, route_weights.T, out_weight, gate_proj, up_proj, down_proj,
    )


def solution(mesh):
    placed = (
        P("ep", "tp"), P("ep", "tp"), P("ep", "tp"), P("ep", "tp"), P("ep", "tp"),
        P(None, "tp"), P("ep", None), P(), P("ep", None), P("ep", None),
        P("ep", None, "tp"), P("ep", None, "tp"), P("ep", None, "tp"),
    )
    return jax.shard_map(
        functools.partial(on_device, mesh.shape["ep"], mesh.shape["tp"]),
        mesh=mesh, in_specs=placed, out_specs=(P("ep", "tp"), P("ep", "tp")), check_vma=False,
    )
```

```python
import functools

import jax
import jax.numpy as jnp
import numpy as np
from jax import lax
from jax.experimental import pallas as pl
from jax.experimental.pallas import tpu as pltpu
from jax.sharding import PartitionSpec as P

BLOCK = 128
MESH = pl.DeviceIdType.MESH
F32 = jnp.float32
BF16 = jnp.bfloat16


def each(low, high, body):
    if high - low <= 8:
        for index in range(low, high):
            body(index)
    else:

        @pl.loop(low, high)
        def _(index):
            body(index)


def span(index, size):
    return pl.ds(pl.multiple_of(index * size, size), size)


def split(value):
    high = value.astype(BF16)
    return high, (value - high.astype(F32)).astype(BF16)


def dot(a, b, dims=((1,), (0,))):
    return lax.dot_general(a, b, (dims, ((), ())), preferred_element_type=F32)


def chunk_units(ep):
    g = ep // 4
    return [(0, g), (2 * g, g), (g, g), (3 * g, g // 2), (3 * g + g // 2, g // 2)]


class Gather:
    def __init__(self, tp, region, half, send, recv):
        self.tp, self.region, self.half, self.send, self.recv = tp, region, half, send, recv
        self.me = lax.axis_index("tp")

    def copy(self, ref, slot, to):
        return pltpu.make_async_remote_copy(
            src_ref=ref, dst_ref=ref, send_sem=self.send(slot), recv_sem=self.recv(slot),
            device_id={"tp": to}, device_id_type=MESH,
        )

    def outs(self):
        me, tp = self.me, self.tp
        if tp == 4:
            return [self.copy(self.region(me), k - 1, me ^ k) for k in (1, 2)]
        return [self.copy(self.region(me), k - 1, lax.rem(me + k, tp)) for k in range(1, tp)]

    def hops(self):
        me = self.me
        return [
            self.copy(self.half(me ^ 1, 0), 2, me ^ 2),
            self.copy(self.half(me ^ 2, 1), 3, me ^ 1),
        ]

    def start(self):
        for copy in self.outs():
            copy.start()

    def forward(self):
        if self.tp == 4:
            me = self.me
            hops = self.hops()
            for k in (1, 2):
                self.copy(self.region(me ^ k), k - 1, me ^ k).wait_recv()
                hops[k - 1].start()

    def finish(self):
        me, tp = self.me, self.tp
        if tp == 4:
            self.copy(self.half(me ^ 3, 0), 2, me ^ 2).wait_recv()
            self.copy(self.half(me ^ 3, 1), 3, me ^ 1).wait_recv()
        else:
            for k in range(1, tp):
                owner = lax.rem(me + tp - k, tp)
                self.copy(self.region(owner), k - 1, owner).wait_recv()

    def drain(self):
        for copy in self.outs() + (self.hops() if self.tp == 4 else []):
            copy.wait_send()


def kernel(
    ep, tp,
    q_hbm, k_hbm, v_hbm, g_hbm, ld_hbm, tab_hbm, rows_hbm, gain_hbm, routes_hbm, rw_hbm,
    wo_hbm, wg_hbm, wu_hbm, wd_hbm,
    out_ref,
    ld_ref, gain_ref, routes_ref, rw_ref, q_ref, k_ref, v_ref, g_ref, tab, rows_ref, turn,
    wo, wg, wu, wd, normed, p0, p1, og, x, h, eo, ret, ho, state, landed, excl,
    rq, inside, cums, pack, narrow,
    w_sem, z_send, z_recv, f_send, f_recv, h_send, h_recv, r_send, r_recv, m_send, m_recv,
    s_send, s_recv,
):

    e, t = lax.axis_index("ep"), lax.axis_index("tp")
    rows, d = rows_ref.shape
    cap = 2 * rows // ep
    dq = d // tp
    ff = wd.shape[0]
    fq = ff // tp
    heads = ld_ref.shape[0]
    hd = q_ref.shape[1] // heads
    blocks = rows // BLOCK
    g = ep // 4
    units = chunk_units(ep)
    tile = min(256, fq)
    pieces = 2 if fq >= 512 else 1
    piece = fq // pieces
    core, chip, chips = lax.rem(e, 2), e // 2, ep // 2

    barrier = pltpu.get_barrier_semaphore()

    def greet_ep(off):
        pl.semaphore_signal(barrier, inc=1, device_id={"ep": e ^ off}, device_id_type=MESH)

    each(1, ep, greet_ep)
    for k in range(1, tp):
        pl.semaphore_signal(
            barrier, inc=1, device_id={"tp": lax.rem(t + k, tp)}, device_id_type=MESH
        )

    parts = 2
    step_rows = rows // parts
    part_at = [slice(i * step_rows, (i + 1) * step_rows) for i in range(parts)]
    row_loads = [
        pltpu.make_async_copy(rows_hbm.at[at, :], rows_ref.at[at, :], w_sem.at[7 + i])
        for i, at in enumerate(part_at)
    ]
    loads = [
        pltpu.make_async_copy(src, dst, w_sem.at[i])
        for i, (src, dst) in enumerate(
            (
                (wd_hbm.at[0], wd), (wo_hbm, wo),
                (q_hbm, q_ref), (k_hbm, k_ref), (v_hbm, v_ref), (g_hbm, g_ref), (tab_hbm, tab),
            )
        )
    ]
    weight_loads = [
        [
            pltpu.make_async_copy(
                src.at[0, :, j * piece : (j + 1) * piece], dst.at[:, j * piece : (j + 1) * piece],
                w_sem.at[9 + 2 * j + i],
            )
            for i, (src, dst) in enumerate(((wg_hbm, wg), (wu_hbm, wu)))
        ]
        for j in range(pieces)
    ]
    small_loads = [
        pltpu.make_async_copy(src, dst, w_sem.at[13 + i])
        for i, (src, dst) in enumerate(
            (
                (routes_hbm, routes_ref), (gain_hbm, gain_ref), (ld_hbm, ld_ref), (rw_hbm, rw_ref),
            )
        )
    ]
    for load in row_loads + small_loads + sum(weight_loads, []):
        load.start()

    small_loads[0].wait()
    routes = [routes_ref[k : k + 1, :] for k in range(2)]
    experts = lax.broadcasted_iota(jnp.int32, (max(8, ep), rows), 0)
    hot = [(experts == routes[k]).astype(F32) for k in range(2)]
    before = (
        lax.broadcasted_iota(jnp.int32, (rows, rows), 0)
        < lax.broadcasted_iota(jnp.int32, (rows, rows), 1)
    ).astype(F32).astype(BF16)
    rank = dot((hot[0] + hot[1]).astype(BF16), before)
    targets = [
        routes[k] * cap + jnp.sum(rank * hot[k], axis=0, keepdims=True).astype(jnp.int32)
        for k in range(2)
    ]

    small_loads[1].wait()
    for i, at in enumerate(part_at):
        row_loads[i].wait()
        squares = None
        for c in range(d // 128):
            val = rows_ref[at, c * 128 : (c + 1) * 128].astype(F32)
            squares = val * val if squares is None else squares + val * val
        scale = lax.rsqrt(jnp.sum(squares, axis=-1, keepdims=True) / d + 1e-06)
        for c in range(d // 128):
            cols = slice(c * 128, (c + 1) * 128)
            val = rows_ref[at, cols].astype(F32)
            normed[at, cols] = (val * scale * gain_ref[c : c + 1, :].astype(F32)).astype(BF16)

    def unit_at(low, size):
        return span((e // size) ^ (low // size), size * cap)

    def pick(low, size):
        slot = lax.broadcasted_iota(jnp.int32, (size * cap, rows), 0) + (
            (e // size) ^ (low // size)
        ) * (size * cap)
        return ((slot == targets[0]) | (slot == targets[1])).astype(F32).astype(BF16)

    def group(low, size, start, width):
        chosen = pick(low, size)
        wide = min(256, width)
        for c in range(width // wide):
            cols = pl.ds(pl.multiple_of(start + c * wide, wide), wide)
            og[unit_at(low, size), cols] = dot(chosen, normed[:, cols]).astype(BF16)

    group(0, g, 0, d)
    group(2 * g, g, t * dq, dq)
    pl.semaphore_wait(barrier, ep - 1 + tp - 1)

    def z_copy(off, here, whole):
        other = e ^ off
        land = span(other if here else e, cap)
        if whole:
            src, dst = og.at[span(other, cap), :], x.at[land, :]
        else:
            src, dst = og.at[span(other, cap), span(t, dq)], x.at[land, span(t, dq)]
        return pltpu.make_async_remote_copy(
            src_ref=src, dst_ref=dst, send_sem=z_send.at[other],
            recv_sem=z_recv.at[other if here else e],
            device_id={"ep": other}, device_id_type=MESH,
        )

    slim = [(2, g), (2 * g, 3 * g)]
    full = [(g, 2 * g), (3 * g, 4 * g)]

    def z_start(low, high, whole):
        each(low, high, lambda off: z_copy(off, False, whole).start())

    z_start(1, 2, True)
    for low, high in slim:
        z_start(low, high, False)
    for load in loads[2:7] + loads[0:2]:
        load.start()
    x[span(e, cap), :] = og[span(e, cap), :]
    for low, high in full:
        group(low, high - low, 0, d)

    @pl.when(core == 0)
    def _():
        z_start(*full[0], True)


    def row_gather(off):
        other = e ^ off
        start = other * cap

        def half(owner, k):
            return x.at[
                pl.ds(pl.multiple_of(start + k * (cap // 2), cap // 2), cap // 2), span(owner, dq)
            ]

        return Gather(
            tp, lambda owner: x.at[span(other, cap), span(owner, dq)], half,
            lambda slot: f_send.at[other, slot], lambda slot: f_recv.at[other, slot],
        )

    def hid_gather(u, j):
        low, size = units[u]
        count = size * cap
        base = ((e // size) ^ (low // size)) * count

        def cols(owner):
            return pl.ds(pl.multiple_of(owner * fq + j * piece, piece), piece)

        return Gather(
            tp,
            lambda owner: h.at[pl.ds(pl.multiple_of(base, count), count), cols(owner)],
            lambda owner, k: h.at[
                pl.ds(pl.multiple_of(base + k * (count // 2), count // 2), count // 2), cols(owner)
            ],
            lambda slot: h_send.at[u * pieces + j, slot],
            lambda slot: h_recv.at[u * pieces + j, slot],
        )

    half_rows = rows // 2

    def mix_gather(b):
        def at(low, size):
            return slice(b * half_rows + low, b * half_rows + low + size)

        return Gather(
            tp, lambda owner: ho.at[at(0, half_rows), span(owner, heads * hd)],
            lambda owner, k: ho.at[
                at(k * (half_rows // 2), half_rows // 2), span(owner, heads * hd)
            ],
            lambda slot: m_send.at[b, slot], lambda slot: m_recv.at[b, slot],
        )

    def take_rows(off):
        z_copy(off, True, False).wait_recv()
        row_gather(off).start()

    def hidden_piece(u, j):
        at = unit_at(*units[u])

        @pl.loop(0, piece // tile)
        def _(i):
            cols = pl.ds(pl.multiple_of(j * piece + i * tile, tile), tile)
            held = x[at, :]
            gate = dot(held, wg[:, cols])
            up = dot(held, wu[:, cols])
            hid = (gate / (1.0 + jnp.exp(-gate)) * up).astype(BF16)
            h[at, pl.ds(pl.multiple_of(t * fq + j * piece + i * tile, tile), tile)] = hid

        hid_gather(u, j).start()

    def back_copy(off, here):
        other = e ^ off
        return pltpu.make_async_remote_copy(
            src_ref=eo.at[span(other, cap), :], dst_ref=ret.at[span(other if here else e, cap), :],
            send_sem=r_send.at[other], recv_sem=r_recv.at[other if here else e],
            device_id={"ep": other}, device_id_type=MESH,
        )

    out_tile = min(256, dq)

    def down(u):
        for j in range(pieces):
            hid_gather(u, j).finish()
        low, size = units[u]
        at = unit_at(low, size)

        @pl.loop(0, dq // out_tile)
        def _(i):
            cols = pl.ds(pl.multiple_of(i * out_tile, out_tile), out_tile)
            eo[at, cols] = dot(h[at, :], wd[:, cols]).astype(BF16)

        each(max(1, low), low + size, lambda off: back_copy(off, False).start())
        if low == 0:
            ret[span(e, cap), :] = eo[span(e, cap), :]

    def forward(u, j):
        hid_gather(u, j).forward()

    row_i = lax.broadcasted_iota(jnp.int32, (BLOCK, BLOCK), 0)
    col_j = lax.broadcasted_iota(jnp.int32, (BLOCK, BLOCK), 1)
    causal = row_i >= col_j
    lower = causal.astype(F32)
    factor = hd ** (-0.5)
    decay_at = heads * hd

    def retention_local():
        small_loads[2].wait()
        small_loads[3].wait()
        pack[...] = jnp.zeros_like(pack)
        pack[0:1, :] = targets[0].astype(F32)
        pack[1:2, :] = targets[1].astype(F32)
        pack[2:4, :] = rw_ref[...]
        pack[4 : 4 + heads, :] = ld_ref[...]
        for b in range(rows // 128):
            narrow[b * 128 : (b + 1) * 128, :] = pack[:, b * 128 : (b + 1) * 128].T
        lanes = lax.broadcasted_iota(jnp.int32, (rows, ep * cap), 1)
        for k, ref in ((0, p0), (1, p1)):
            ref[...] = (lanes == narrow[:, k : k + 1].astype(jnp.int32)).astype(F32).astype(BF16)
        for load in loads[2:7]:
            load.wait()
        here_cos = tab[pl.ds(2 * rows + e, 1), :]
        here_sin = tab[pl.ds(2 * rows + ep + e, 1), :]
        sign = jnp.where(lax.broadcasted_iota(jnp.int32, (BLOCK, hd), 1) < hd // 2, -1.0, 1.0)
        for b in range(blocks):
            at = slice(b * BLOCK, (b + 1) * BLOCK)
            cos, sin = tab[at, :], tab[slice(rows + b * BLOCK, rows + (b + 1) * BLOCK), :]
            turn[0, at, :] = cos * here_cos - sin * here_sin
            turn[1, at, :] = (sin * here_cos + cos * here_sin) * sign
            cums[at, :] = lax.dot_general(
                lower, narrow[at, :], (((1,), (0,)), ((), ())),
                preferred_element_type=F32, precision=lax.Precision.HIGHEST,
            )
        for n in range(heads):
            cols = slice(n * hd, (n + 1) * hd)
            total = None
            gone = None
            for b in range(blocks):
                at = slice(b * BLOCK, (b + 1) * BLOCK)
                cos, sin = turn[0, at, :], turn[1, at, :]

                def turned(ref):
                    val = ref[at, cols].astype(F32)
                    return val * cos + pltpu.roll(val, hd // 2, 1) * sin

                qb = turned(q_ref).astype(BF16)
                kb = (turned(k_ref) * factor).astype(BF16)
                vb = v_ref[at, cols]
                rq[at, cols] = qb
                cum = jnp.broadcast_to(cums[at, 4 + n : 5 + n], (BLOCK, BLOCK))
                spread = cum - cum.T
                weight = jnp.where(causal, jnp.exp(jnp.where(causal, spread, 0.0)), 0.0)
                scores = dot(qb, kb, ((1,), (1,)))
                inside[at, cols] = dot((scores * weight).astype(BF16), vb)
                ending = cum[BLOCK - 1 : BLOCK, :]
                k_hi, k_lo = split(kb.astype(F32) * jnp.exp(ending - cum))
                update = dot(k_hi, vb, ((0,), (0,))) + dot(k_lo, vb, ((0,), (0,)))
                if b == 0:
                    total, gone = update, ending
                else:
                    total = jnp.exp(ending) * total + update
                    gone = gone + ending
                if b < blocks - 1:
                    excl[1 + b, n * hd : (n + 1) * hd, :] = total
            state[0, n * hd : (n + 1) * hd, :] = total
            state[0, decay_at + n : decay_at + n + 1, :] = jnp.exp(gone)
        excl[0, :decay_at, :] = jnp.zeros((decay_at, hd), F32)

    def up_copy():
        return pltpu.make_async_remote_copy(
            src_ref=state.at[0], dst_ref=landed.at[0], send_sem=s_send.at[0],
            recv_sem=s_recv.at[0], device_id={"ep": e ^ 1}, device_id_type=MESH,
        )

    def next_copy():
        return pltpu.make_async_remote_copy(
            src_ref=state.at[1, :decay_at, :], dst_ref=landed.at[1, :decay_at, :],
            send_sem=s_send.at[1], recv_sem=s_recv.at[1],
            device_id={"ep": lax.rem(e + 2, ep)}, device_id_type=MESH,
        )

    def down_copy():
        part = landed.at[1, :decay_at, :]
        return pltpu.make_async_remote_copy(
            src_ref=part, dst_ref=part, send_sem=s_send.at[2], recv_sem=s_recv.at[2],
            device_id={"ep": e ^ 1}, device_id_type=MESH,
        )

    def decays(n):
        at = slice(decay_at + n, decay_at + n + 1)
        return landed[0, at, :], state[0, at, :]

    def scan_open():
        @pl.when(core == 1)
        def _():
            up_copy().wait_recv()
            for n in range(heads):
                at = slice(n * hd, (n + 1) * hd)
                mine = decays(n)[1]
                state[1, at, :] = mine * landed[0, at, :] + state[0, at, :]
                excl[0, at, :] = landed[0, at, :]

        if chips > 1:

            @pl.when((core == 1) & (chip == 0))
            def _():
                next_copy().start()

    def scan_pass(turn_of):
        @pl.when((core == 1) & turn_of)
        def _():
            next_copy().wait_recv()
            down_copy().start()
            for n in range(heads):
                at = slice(n * hd, (n + 1) * hd)
                first, mine = decays(n)
                came = landed[1, at, :]
                state[1, at, :] = (first * mine) * came + state[1, at, :]
                excl[0, at, :] = first * came + excl[0, at, :]

        @pl.when((core == 1) & turn_of & (chip < chips - 1))
        def _():
            next_copy().start()

    def scan_close():
        @pl.when((core == 0) & (chip > 0))
        def _():
            down_copy().wait_recv()
            excl[0, :decay_at, :] = landed[1, :decay_at, :]

    def retention_close():
        for n in range(heads):
            cols = slice(n * hd, (n + 1) * hd)
            sat = slice(n * hd, (n + 1) * hd)
            entering = excl[0, sat, :]
            gone = None
            for b in range(blocks):
                at = slice(b * BLOCK, (b + 1) * BLOCK)
                cum = jnp.broadcast_to(cums[at, 4 + n : 5 + n], (BLOCK, hd))
                held = entering if b == 0 else jnp.exp(gone) * entering + excl[b, sat, :]
                hi, lo = split(held)
                qb = rq[at, cols]
                retained = inside[at, cols] + (dot(qb, hi) + dot(qb, lo)) * jnp.exp(cum)
                scale = lax.rsqrt(jnp.mean(retained * retained, axis=-1, keepdims=True) + 1e-05)
                gate = g_ref[at, cols].astype(F32)
                out = (retained * scale * (gate / (1.0 + jnp.exp(-gate)))).astype(BF16)
                ho[at, pl.ds(pl.multiple_of(t * heads * hd + n * hd, hd), hd)] = out
                ending = cum[BLOCK - 1 : BLOCK, :]
                gone = ending if gone is None else gone + ending

    for load in weight_loads[0]:
        load.wait()
    z_copy(1, True, True).wait_recv()
    each(2, g, take_rows)
    each(2, g, lambda off: row_gather(off).forward())
    each(2, g, lambda off: row_gather(off).finish())
    hidden_piece(0, 0)
    retention_local()

    @pl.when(core == 0)
    def _():
        up_copy().start()

    for j in range(1, pieces):
        for load in weight_loads[j]:
            load.wait()
        hidden_piece(0, j)
    scan_open()
    last = full[1][1] - (full[1][1] - full[1][0]) // 2

    @pl.when(core == 1)
    def _():
        z_start(*full[0], True)
        z_start(full[1][0], last, True)

    @pl.when(core == 0)
    def _():
        z_start(*full[1], True)


    each(2 * g, 3 * g, take_rows)
    each(2 * g, 3 * g, lambda off: row_gather(off).forward())
    for j in range(pieces):
        forward(0, j)
    scan_pass(chip == 1)

    @pl.when(core == 1)
    def _():
        z_start(last, full[1][1], True)

    each(2 * g, 3 * g, lambda off: row_gather(off).finish())
    for j in range(pieces):
        hidden_piece(1, j)

    each(g, 2 * g, lambda off: z_copy(off, True, True).wait_recv())
    for j in range(pieces):
        hidden_piece(2, j)
    loads[0].wait()
    down(0)
    forward(1, 0)
    scan_pass(chip == 2)
    for j in range(1, pieces):
        forward(1, j)
    forward(2, 0)

    def last_rows(u):
        low, size = units[u]
        each(low, low + size, lambda off: z_copy(off, True, True).wait_recv())
        for j in range(pieces):
            hidden_piece(u, j)

    last_rows(3)
    for j in range(1, pieces):
        forward(2, j)
    scan_pass(chip > 2)
    scan_close()
    retention_close()
    mix_gather(0).start()
    last_rows(4)
    down(1)
    for j in range(pieces):
        forward(3, j)
    down(2)
    mix_gather(0).forward()
    for j in range(pieces):
        forward(4, j)
    mix_gather(1).start()
    down(3)
    down(4)
    mix_gather(1).forward()
    loads[1].wait()

    for b in range(2):
        mix_gather(b).finish()

    @pl.loop(0, dq // out_tile)
    def _(i):
        cols = pl.ds(pl.multiple_of(i * out_tile, out_tile), out_tile)
        out_ref[0, :, cols] = dot(ho[...], wo[:, cols]).astype(BF16)

    each(1, ep, lambda off: back_copy(off, True).wait_recv())

    @pl.loop(0, dq // out_tile)
    def _(i):
        cols = pl.ds(pl.multiple_of(i * out_tile, out_tile), out_tile)
        came = ret[:, cols]
        out_ref[1, :, cols] = (
            dot(p0[...], came) * narrow[:, 2:3] + dot(p1[...], came) * narrow[:, 3:4]
        ).astype(BF16)


    def drain(low, high, whole):
        each(low, high, lambda off: z_copy(off, False, whole).wait_send())

    drain(1, 2, True)
    for low, high in slim:
        drain(low, high, False)
        each(low, high, lambda off: row_gather(off).drain())
    for low, high in full:
        drain(low, high, True)
    each(1, ep, lambda off: back_copy(off, False).wait_send())
    for u in range(len(units)):
        for j in range(pieces):
            hid_gather(u, j).drain()
    for b in range(2):
        mix_gather(b).drain()

    @pl.when(core == 0)
    def _():
        up_copy().wait_send()

    @pl.when((core == 1) & (chip < chips - 1))
    def _():
        next_copy().wait_send()

    @pl.when((core == 1) & (chip > 0))
    def _():
        down_copy().wait_send()


def turn_table(ep, rows, hd):
    half = hd // 2
    inverse = np.tile(10000.0 ** (-np.arange(half) / half), 2)
    near = np.arange(rows)[:, None] * inverse[None, :]
    far = (np.arange(ep) * rows)[:, None] * inverse[None, :]
    parts = [np.cos(near), np.sin(near), np.cos(far), np.sin(far)]
    return np.concatenate(parts).astype(np.float32)


def on_device(
    ep, tp,
    queries, keys, values, gates, log_decay, out_weight, moe_rows, moe_gain, routes,
    route_weights, gate_proj, up_proj, down_proj,
):
    rows, d = moe_rows.shape
    heads = log_decay.shape[1]
    width = queries.shape[1]
    hd = width // heads
    cap = 2 * rows // ep
    dq = d // tp
    fq = gate_proj.shape[2]
    ff = down_proj.shape[1]
    slots = max(4, tp - 1)
    pieces = len(chunk_units(ep)) * 2
    blocks = rows // BLOCK
    srows = heads * hd + 8 * ((heads + 7) // 8)
    vmem = pl.BlockSpec(memory_space=pltpu.VMEM)
    dma = pltpu.SemaphoreType.DMA
    table = jnp.asarray(turn_table(ep, rows, hd))
    operands = [
        pltpu.with_memory_space_constraint(operand, pltpu.HBM)
        for operand in (
            queries, keys, values, gates, log_decay.T, table, moe_rows, moe_gain.reshape(-1, 128),
            routes.T, route_weights.T, out_weight, gate_proj, up_proj, down_proj,
        )
    ]
    both = pl.pallas_call(
        functools.partial(kernel, ep, tp),
        out_shape=jax.ShapeDtypeStruct((2, rows, dq), BF16),
        in_specs=[pl.BlockSpec(memory_space=pltpu.HBM)] * 14,
        out_specs=vmem,
        scratch_shapes=[
            pltpu.VMEM((heads, rows), F32),
            pltpu.VMEM((d // 128, 128), BF16),
            pltpu.VMEM((2, rows), jnp.int32),
            pltpu.VMEM((2, rows), F32),
            pltpu.VMEM((rows, width), BF16),
            pltpu.VMEM((rows, width), BF16),
            pltpu.VMEM((rows, width), BF16),
            pltpu.VMEM((rows, width), BF16),
            pltpu.VMEM(table.shape, F32),
            pltpu.VMEM((rows, d), BF16),
            pltpu.VMEM((2, rows, hd), F32),
            pltpu.VMEM(out_weight.shape, BF16),
            pltpu.VMEM((d, fq), BF16),
            pltpu.VMEM((d, fq), BF16),
            pltpu.VMEM((ff, dq), BF16),
            pltpu.VMEM((rows, d), BF16),
            pltpu.VMEM((rows, ep * cap), BF16),
            pltpu.VMEM((rows, ep * cap), BF16),
            pltpu.VMEM((ep * cap, d), BF16),
            pltpu.VMEM((ep * cap, d), BF16),
            pltpu.VMEM((ep * cap, ff), BF16),
            pltpu.VMEM((ep * cap, dq), BF16),
            pltpu.VMEM((ep * cap, dq), BF16),
            pltpu.VMEM((rows, width * tp), BF16),
            pltpu.VMEM((2, srows, hd), F32),
            pltpu.VMEM((2, srows, hd), F32),
            pltpu.VMEM((blocks, srows, hd), F32),
            pltpu.VMEM((rows, width), BF16),
            pltpu.VMEM((rows, width), F32),
            pltpu.VMEM((rows, 128), F32),
            pltpu.VMEM((128, rows), F32),
            pltpu.VMEM((rows, 128), F32),
            dma((17,)),
            dma((ep,)), dma((ep,)),
            dma((ep, slots)), dma((ep, slots)),
            dma((pieces, slots)), dma((pieces, slots)),
            dma((ep,)), dma((ep,)),
            dma((2, slots)), dma((2, slots)),
            dma((3,)), dma((3,)),
        ],
        compiler_params=pltpu.CompilerParams(
            collective_id=0, has_side_effects=True, vmem_limit_bytes=44 * 1024 * 1024
        ),
    )(*operands)
    return both[0], both[1]


def solution(mesh):
    placed = (
        P("ep", "tp"), P("ep", "tp"), P("ep", "tp"), P("ep", "tp"), P("ep", "tp"),
        P(None, "tp"), P("ep", None), P(), P("ep", None), P("ep", None),
        P("ep", None, "tp"), P("ep", None, "tp"), P("ep", None, "tp"),
    )
    return jax.shard_map(
        functools.partial(on_device, mesh.shape["ep"], mesh.shape["tp"]),
        mesh=mesh, in_specs=placed, out_specs=(P("ep", "tp"), P("ep", "tp")), check_vma=False,
    )
```

```python
import functools

import jax
import jax.numpy as jnp
import numpy as np
from jax import lax
from jax.experimental import pallas as pl
from jax.experimental.pallas import tpu as pltpu
from jax.sharding import PartitionSpec as P

BLOCK = 128
MESH = pl.DeviceIdType.MESH
F32 = jnp.float32
BF16 = jnp.bfloat16


def each(low, high, body):
    if high - low <= 8:
        for index in range(low, high):
            body(index)
    else:

        @pl.loop(low, high)
        def _(index):
            body(index)


def span(index, size):
    return pl.ds(pl.multiple_of(index * size, size), size)


def split(value):
    high = value.astype(BF16)
    return high, (value - high.astype(F32)).astype(BF16)


def dot(a, b, dims=((1,), (0,))):
    return lax.dot_general(a, b, (dims, ((), ())), preferred_element_type=F32)


def plan(ep):
    q = ep // 8
    order = ((0, False), (1, False), (4, False), (6, False), (2, True), (5, True), (7, True), (3, True))
    return [(low * q, q, whole) for low, whole in order]


class Gather:
    def __init__(self, tp, region, half, send, recv, hop):
        self.tp, self.region, self.half, self.send = tp, region, half, send
        self.recv, self.hop = recv, hop
        self.me = lax.axis_index("tp")

    def copy(self, ref, recv, to):
        return pltpu.make_async_remote_copy(
            src_ref=ref, dst_ref=ref, send_sem=self.send, recv_sem=recv,
            device_id={"tp": to}, device_id_type=MESH,
        )

    def start(self):
        me, tp = self.me, self.tp
        if tp == 4:
            for k in (1, 2):
                self.copy(self.region(me), self.recv(k - 1), me ^ k).start()
        else:
            for k in range(1, tp):
                self.copy(self.region(me), self.recv(k - 1), lax.rem(me + k, tp)).start()

    def forward(self):
        if self.tp == 4:
            me = self.me
            for k in (1, 2):
                self.copy(self.region(me ^ k), self.recv(k - 1), me ^ k).wait_recv()
                self.copy(self.half(me ^ k, k - 1), self.hop, me ^ (3 - k)).start()

    def finish(self):
        me, tp = self.me, self.tp
        if tp == 4:
            self.copy(self.region(me ^ 3), self.hop, me ^ 3).wait_recv()
        else:
            for k in range(1, tp):
                owner = lax.rem(me + tp - k, tp)
                self.copy(self.region(owner), self.recv(k - 1), owner).wait_recv()


def kernel(
    ep, tp,
    q_hbm, k_hbm, v_hbm, g_hbm, ld_hbm, tab_hbm, rows_hbm, gain_hbm, routes_hbm, rw_hbm,
    wo_hbm, wg_hbm, wu_hbm, wd_hbm,
    out_ref,
    ld_ref, gain_ref, routes_ref, rw_ref, heads_in, tab, rows_ref, turn,
    wo, wg, wu, wd, normed, p0, p1, og, x, h, eo, ret, ho, state, landed, passed, excl, partial,
    rq, inside, cums, pack, narrow,
    w_sem, sent, z_recv, f_recv, f_hop, h_recv, h_hop, r_recv, m_recv, m_hop, s_send, s_recv,
):

    e, t = lax.axis_index("ep"), lax.axis_index("tp")
    rows, d = rows_ref.shape
    cap = 2 * rows // ep
    dq = d // tp
    ff = wd.shape[0]
    fq = ff // tp
    heads = ld_ref.shape[0]
    hd = heads_in.shape[2] // heads
    q_ref, k_ref, v_ref, g_ref = [heads_in.at[i] for i in range(4)]
    blocks = rows // BLOCK
    g = ep // 4
    units = plan(ep)
    tile = min(256, fq)
    pieces = 2 if fq >= 512 else 1
    piece = fq // pieces
    cuts = [(j * piece, piece) for j in range(pieces)]
    first = [(0, tile), (tile, piece - tile)] * (piece > tile) + cuts[piece > tile :]
    core, chip, chips = lax.rem(e, 2), e // 2, ep // 2

    barrier = pltpu.get_barrier_semaphore()

    def greet_ep(off):
        pl.semaphore_signal(barrier, inc=1, device_id={"ep": e ^ off}, device_id_type=MESH)

    each(1, ep, greet_ep)
    for k in range(1, tp):
        pl.semaphore_signal(
            barrier, inc=1, device_id={"tp": lax.rem(t + k, tp)}, device_id_type=MESH
        )

    parts = 2
    step_rows = rows // parts
    part_at = [slice(i * step_rows, (i + 1) * step_rows) for i in range(parts)]
    row_loads = [
        pltpu.make_async_copy(rows_hbm.at[at, :], rows_ref.at[at, :], w_sem.at[4 + i])
        for i, at in enumerate(part_at)
    ]
    loads = [
        pltpu.make_async_copy(src, dst, w_sem.at[i])
        for i, (src, dst) in enumerate(
            (
                (wd_hbm.at[0], wd), (wo_hbm, wo), (tab_hbm, tab),
            )
        )
    ]
    head_loads = [
        pltpu.make_async_copy(src, dst, w_sem.at[3])
        for src, dst in ((q_hbm, q_ref), (k_hbm, k_ref), (v_hbm, v_ref), (g_hbm, g_ref))
    ]
    weight_loads = [
        [
            pltpu.make_async_copy(
                src.at[0, :, j * piece : (j + 1) * piece], dst.at[:, j * piece : (j + 1) * piece],
                w_sem.at[6 + 2 * j + i],
            )
            for i, (src, dst) in enumerate(((wg_hbm, wg), (wu_hbm, wu)))
        ]
        for j in range(pieces)
    ]
    small_loads = [
        pltpu.make_async_copy(src, dst, w_sem.at[10 + i])
        for i, (src, dst) in enumerate(
            (
                (routes_hbm, routes_ref), (gain_hbm, gain_ref), (ld_hbm, ld_ref), (rw_hbm, rw_ref),
            )
        )
    ]
    for load in row_loads + small_loads + sum(weight_loads, []):
        load.start()

    small_loads[0].wait()
    routes = [routes_ref[k : k + 1, :] for k in range(2)]
    experts = lax.broadcasted_iota(jnp.int32, (max(8, ep), rows), 0)
    hot = [(experts == routes[k]).astype(F32) for k in range(2)]
    before = (
        lax.broadcasted_iota(jnp.int32, (rows, rows), 0)
        < lax.broadcasted_iota(jnp.int32, (rows, rows), 1)
    ).astype(F32).astype(BF16)
    rank = dot((hot[0] + hot[1]).astype(BF16), before)
    targets = [
        routes[k] * cap + jnp.sum(rank * hot[k], axis=0, keepdims=True).astype(jnp.int32)
        for k in range(2)
    ]

    small_loads[1].wait()
    for i, at in enumerate(part_at):
        row_loads[i].wait()
        squares = None
        for c in range(d // 128):
            val = rows_ref[at, c * 128 : (c + 1) * 128].astype(F32)
            squares = val * val if squares is None else squares + val * val
        scale = lax.rsqrt(jnp.sum(squares, axis=-1, keepdims=True) / d + 1e-06)
        for c in range(d // 128):
            cols = slice(c * 128, (c + 1) * 128)
            val = rows_ref[at, cols].astype(F32)
            normed[at, cols] = (val * scale * gain_ref[c : c + 1, :].astype(F32)).astype(BF16)

    def unit_at(low, size):
        return span((e // size) ^ (low // size), size * cap)

    def pick(low, size):
        slot = lax.broadcasted_iota(jnp.int32, (size * cap, rows), 0) + (
            (e // size) ^ (low // size)
        ) * (size * cap)
        return ((slot == targets[0]) | (slot == targets[1])).astype(F32).astype(BF16)

    def group(low, size, start, width):
        chosen = pick(low, size)
        wide = min(256, width)
        for c in range(width // wide):
            cols = pl.ds(pl.multiple_of(start + c * wide, wide), wide)
            og[unit_at(low, size), cols] = dot(chosen, normed[:, cols]).astype(BF16)

    group(0, g, 0, d)
    for low, size, whole in units[2:4]:
        group(low, size, t * dq, dq)
    pl.semaphore_wait(barrier, ep - 1 + tp - 1)

    def z_copy(off, here, whole):
        other = e ^ off
        land = span(other if here else e, cap)
        if whole:
            src, dst = og.at[span(other, cap), :], x.at[land, :]
        else:
            src, dst = og.at[span(other, cap), span(t, dq)], x.at[land, span(t, dq)]
        return pltpu.make_async_remote_copy(
            src_ref=src, dst_ref=dst, send_sem=sent.at[0 if whole else 1],
            recv_sem=z_recv.at[other if here else e],
            device_id={"ep": other}, device_id_type=MESH,
        )

    def offsets(u):
        low, size, whole = units[u]
        return max(2, low), max(2, low + size), whole

    def z_start(u):
        low, high, whole = offsets(u)
        each(low, high, lambda off: z_copy(off, False, whole).start())

    def z_wait(u):
        low, high, whole = offsets(u)
        each(low, high, lambda off: z_copy(off, True, whole).wait_recv())

    z_copy(1, False, True).start()
    for u in range(4):
        z_start(u)
    for load in head_loads + loads[2:3] + loads[0:2]:
        load.start()
    x[span(e, cap), :] = og[span(e, cap), :]
    group(*units[4][:2], 0, d)
    opens = (core == 1) & (chip == 0)

    @pl.when(jnp.logical_not(opens))
    def _():
        z_start(4)


    slim_at, count = [], 0
    for u in range(4):
        low, high, _ = offsets(u)
        slim_at.append(count - low)
        count += high - low

    def row_gather(u, off):
        other = e ^ off
        start = other * cap
        at = slim_at[u] + off

        def half(owner, k):
            return x.at[
                pl.ds(pl.multiple_of(start + k * (cap // 2), cap // 2), cap // 2), span(owner, dq)
            ]

        return Gather(
            tp, lambda owner: x.at[span(other, cap), span(owner, dq)], half,
            sent.at[2], lambda slot: f_recv.at[at, slot], f_hop.at[at],
        )

    def rows_start(u):
        low, high, _ = offsets(u)

        def take(off):
            z_copy(off, True, False).wait_recv()
            row_gather(u, off).start()

        each(low, high, take)

    def rows_forward(u):
        low, high, _ = offsets(u)
        each(low, high, lambda off: row_gather(u, off).forward())

    def rows_finish(u):
        low, high, _ = offsets(u)
        each(low, high, lambda off: row_gather(u, off).finish())

    def hid_gather(u, number):
        start, width = (0, fq) if number is None else (first if u in (0, 2) else cuts)[number]
        low, size, _ = units[u]
        count = size * cap
        base = ((e // size) ^ (low // size)) * count

        def cols(owner):
            return pl.ds(pl.multiple_of(owner * fq + start, tile), width)

        return Gather(
            tp,
            lambda owner: h.at[pl.ds(pl.multiple_of(base, count), count), cols(owner)],
            lambda owner, k: h.at[
                pl.ds(pl.multiple_of(base + k * (count // 2), count // 2), count // 2), cols(owner)
            ],
            sent.at[3], lambda slot: h_recv.at[u * 3 + number, slot], h_hop.at[u],
        )

    def hid_finish(u):
        if tp == 4:
            hid_gather(u, None).finish()
        else:
            for j in range(len(first if u in (0, 2) else cuts)):
                hid_gather(u, j).finish()

    half_rows = rows // 2

    def mix_gather(b):
        def at(low, size):
            return slice(b * half_rows + low, b * half_rows + low + size)

        return Gather(
            tp, lambda owner: ho.at[at(0, half_rows), span(owner, heads * hd)],
            lambda owner, k: ho.at[
                at(k * (half_rows // 2), half_rows // 2), span(owner, heads * hd)
            ],
            sent.at[4], lambda slot: m_recv.at[b, slot], m_hop.at[b],
        )

    def hidden_piece(u, j):
        at = unit_at(*units[u][:2])
        start, width = (first if u in (0, 2) else cuts)[j]

        @pl.loop(0, width // tile)
        def _(i):
            cols = pl.ds(pl.multiple_of(start + i * tile, tile), tile)
            held = x[at, :]
            gate = dot(held, wg[:, cols])
            up = dot(held, wu[:, cols])
            hid = (gate / (1.0 + jnp.exp(-gate)) * up).astype(BF16)
            h[at, pl.ds(pl.multiple_of(t * fq + start + i * tile, tile), tile)] = hid

        hid_gather(u, j).start()

    def back_copy(off, cols):
        other = e ^ off
        return pltpu.make_async_remote_copy(
            src_ref=eo.at[span(other, cap), cols], dst_ref=ret.at[span(e, cap), cols],
            send_sem=sent.at[5], recv_sem=r_recv.at[0],
            device_id={"ep": other}, device_id_type=MESH,
        )

    out_tile = min(256, dq)

    def down_early(u):
        if tp == 4:
            at = unit_at(*units[u][:2])

            @pl.loop(0, dq // out_tile)
            def _(i):
                cols = pl.ds(pl.multiple_of(i * out_tile, out_tile), out_tile)
                partial[u % 2, :, cols] = sum(
                    dot(h[at, span(t ^ k, fq)], wd[span(t ^ k, fq), cols]) for k in range(3)
                )

    def down(u, early=False):
        hid_finish(u)
        low, size, _ = units[u]
        at = unit_at(low, size)

        @pl.loop(0, dq // out_tile)
        def _(i):
            cols = pl.ds(pl.multiple_of(i * out_tile, out_tile), out_tile)
            if early and tp == 4:
                done = t ^ 3
                total = partial[u % 2, :, cols] + dot(
                    h[at, span(done, fq)], wd[span(done, fq), cols]
                )
            else:
                total = dot(h[at, :], wd[:, cols])
            eo[at, cols] = total.astype(BF16)
            each(max(1, low), low + size, lambda off: back_copy(off, cols).start())

        if low == 0:
            ret[span(e, cap), :] = eo[span(e, cap), :]

    def forward(u, j):
        hid_gather(u, j).forward()

    row_i = lax.broadcasted_iota(jnp.int32, (BLOCK, BLOCK), 0)
    col_j = lax.broadcasted_iota(jnp.int32, (BLOCK, BLOCK), 1)
    causal = row_i >= col_j
    lower = causal.astype(F32)
    factor = hd ** (-0.5)
    decay_at = heads * hd

    def retention_local():
        small_loads[2].wait()
        small_loads[3].wait()
        pack[...] = jnp.zeros_like(pack)
        pack[0:1, :] = targets[0].astype(F32)
        pack[1:2, :] = targets[1].astype(F32)
        pack[2:4, :] = rw_ref[...]
        pack[4 : 4 + heads, :] = ld_ref[...]
        for b in range(rows // 128):
            narrow[b * 128 : (b + 1) * 128, :] = pack[:, b * 128 : (b + 1) * 128].T
        lanes = lax.broadcasted_iota(jnp.int32, (rows, ep * cap), 1)
        for k, ref in ((0, p0), (1, p1)):
            ref[...] = (lanes == narrow[:, k : k + 1].astype(jnp.int32)).astype(F32).astype(BF16)
        loads[2].wait()
        pltpu.make_async_copy(heads_in, heads_in, w_sem.at[3]).wait()
        here_cos = tab[pl.ds(2 * rows + e, 1), :]
        here_sin = tab[pl.ds(2 * rows + ep + e, 1), :]
        sign = jnp.where(lax.broadcasted_iota(jnp.int32, (BLOCK, hd), 1) < hd // 2, -1.0, 1.0)
        for b in range(blocks):
            at = slice(b * BLOCK, (b + 1) * BLOCK)
            cos, sin = tab[at, :], tab[slice(rows + b * BLOCK, rows + (b + 1) * BLOCK), :]
            turn[0, at, :] = cos * here_cos - sin * here_sin
            turn[1, at, :] = (sin * here_cos + cos * here_sin) * sign
            cums[at, :] = lax.dot_general(
                lower, narrow[at, :], (((1,), (0,)), ((), ())),
                preferred_element_type=F32, precision=lax.Precision.HIGHEST,
            )
        for n in range(heads):
            cols = slice(n * hd, (n + 1) * hd)
            total = None
            gone = None
            for b in range(blocks):
                at = slice(b * BLOCK, (b + 1) * BLOCK)
                cos, sin = turn[0, at, :], turn[1, at, :]

                def turned(ref):
                    val = ref[at, cols].astype(F32)
                    return val * cos + pltpu.roll(val, hd // 2, 1) * sin

                qb = turned(q_ref).astype(BF16)
                kb = (turned(k_ref) * factor).astype(BF16)
                vb = v_ref[at, cols]
                rq[at, cols] = qb
                cum = jnp.broadcast_to(cums[at, 4 + n : 5 + n], (BLOCK, BLOCK))
                spread = cum - cum.T
                weight = jnp.where(causal, jnp.exp(jnp.where(causal, spread, 0.0)), 0.0)
                scores = dot(qb, kb, ((1,), (1,)))
                inside[at, cols] = dot((scores * weight).astype(BF16), vb)
                ending = cum[BLOCK - 1 : BLOCK, :]
                k_hi, k_lo = split(kb.astype(F32) * jnp.exp(ending - cum))
                update = dot(k_hi, vb, ((0,), (0,))) + dot(k_lo, vb, ((0,), (0,)))
                if b == 0:
                    total, gone = update, ending
                else:
                    total = jnp.exp(ending) * total + update
                    gone = gone + ending
                if b < blocks - 1:
                    excl[1 + b, n * hd : (n + 1) * hd, :] = total
            state[0, n * hd : (n + 1) * hd, :] = total
            state[0, decay_at + n : decay_at + n + 1, :] = jnp.exp(gone)
        excl[0, :decay_at, :] = jnp.zeros((decay_at, hd), F32)

    def up_copy():
        return pltpu.make_async_remote_copy(
            src_ref=state.at[0], dst_ref=landed.at[0], send_sem=s_send.at[0],
            recv_sem=s_recv.at[0], device_id={"ep": e ^ 1}, device_id_type=MESH,
        )

    def next_copy():
        return pltpu.make_async_remote_copy(
            src_ref=passed.at[0], dst_ref=passed.at[1],
            send_sem=s_send.at[1], recv_sem=s_recv.at[1],
            device_id={"ep": lax.rem(e + 2, ep)}, device_id_type=MESH,
        )

    def down_copy():
        return pltpu.make_async_remote_copy(
            src_ref=passed.at[1], dst_ref=passed.at[1], send_sem=s_send.at[2], recv_sem=s_recv.at[2],
            device_id={"ep": e ^ 1}, device_id_type=MESH,
        )

    def decays(n):
        at = slice(decay_at + n, decay_at + n + 1)
        return landed[0, at, :], state[0, at, :]

    def scan_open():
        @pl.when(core == 1)
        def _():
            up_copy().wait_recv()
            for n in range(heads):
                at = slice(n * hd, (n + 1) * hd)
                mine = decays(n)[1]
                state[1, at, :] = mine * landed[0, at, :] + state[0, at, :]
                excl[0, at, :] = landed[0, at, :]
            passed[0] = state[1, :decay_at, :].astype(BF16)

        if chips > 1:

            @pl.when((core == 1) & (chip == 0))
            def _():
                next_copy().start()

    def scan_pass(turn_of):
        @pl.when((core == 1) & turn_of)
        def _():
            next_copy().wait_recv()
            down_copy().start()
            for n in range(heads):
                at = slice(n * hd, (n + 1) * hd)
                first, mine = decays(n)
                came = passed[1, at, :].astype(F32)
                passed[0, at, :] = ((first * mine) * came + state[1, at, :]).astype(BF16)
                excl[0, at, :] = first * came + excl[0, at, :]

        @pl.when((core == 1) & turn_of & (chip < chips - 1))
        def _():
            next_copy().start()

    def scan_close():
        @pl.when((core == 0) & (chip > 0))
        def _():
            down_copy().wait_recv()
            excl[0, :decay_at, :] = passed[1].astype(F32)

    def retention_close():
        for n in range(heads):
            cols = slice(n * hd, (n + 1) * hd)
            sat = slice(n * hd, (n + 1) * hd)
            entering = excl[0, sat, :]
            gone = None
            for b in range(blocks):
                at = slice(b * BLOCK, (b + 1) * BLOCK)
                cum = jnp.broadcast_to(cums[at, 4 + n : 5 + n], (BLOCK, hd))
                held = entering if b == 0 else jnp.exp(gone) * entering + excl[b, sat, :]
                hi, lo = split(held)
                qb = rq[at, cols]
                retained = inside[at, cols] + (dot(qb, hi) + dot(qb, lo)) * jnp.exp(cum)
                scale = lax.rsqrt(jnp.mean(retained * retained, axis=-1, keepdims=True) + 1e-05)
                gate = g_ref[at, cols].astype(F32)
                out = (retained * scale * (gate / (1.0 + jnp.exp(-gate)))).astype(BF16)
                ho[at, pl.ds(pl.multiple_of(t * heads * hd + n * hd, hd), hd)] = out
                ending = cum[BLOCK - 1 : BLOCK, :]
                gone = ending if gone is None else gone + ending

    for load in weight_loads[0]:
        load.wait()

    def take_partner(u):
        if units[u][0] <= 1 < units[u][0] + units[u][1]:
            z_copy(1, True, True).wait_recv()
        rows_start(u)
        rows_forward(u)
        rows_finish(u)

    def hidden(u):
        for j in range(len(first if u in (0, 2) else cuts)):
            hidden_piece(u, j)

    def forwards(u):
        for j in range(len(first if u in (0, 2) else cuts)):
            forward(u, j)

    take_partner(0)
    for j in range(len(first) - pieces + 1):
        hidden_piece(0, j)
    for j in range(1, pieces):
        for load in weight_loads[j]:
            load.wait()
        hidden_piece(0, j + len(first) - pieces)
    take_partner(1)
    hidden_piece(1, 0)
    retention_local()

    @pl.when(core == 0)
    def _():
        up_copy().start()

    for j in range(len(first) - 1):
        forward(0, j)
    for low, size, whole in units[5:]:
        group(low, size, 0, d)


    @pl.when(jnp.logical_not(opens))
    def _():
        z_start(5)

    @pl.when(core == 0)
    def _():
        z_start(6)

    forward(0, len(first) - 1)
    rows_start(2)
    for j in range(1, pieces):
        hidden_piece(1, j)
    scan_open()

    @pl.when(opens)
    def _():
        z_start(4)
        z_start(5)

    rows_start(3)
    rows_forward(2)
    forward(1, 0)
    rows_forward(3)
    rows_finish(2)
    hidden(2)
    scan_pass(chip == 1)

    @pl.when(core == 1)
    def _():
        z_start(6)

    for j in range(1, pieces):
        forward(1, j)
    rows_finish(3)
    hidden(3)
    loads[0].wait()
    down(0)
    z_wait(4)
    hidden(4)
    forwards(2)
    down(1)
    forwards(3)
    scan_pass(chip == 2)
    z_start(7)
    z_wait(5)
    hidden(5)
    down(2)
    forwards(4)
    down(3)
    scan_pass(chip > 2)
    scan_close()
    retention_close()
    mix_gather(0).start()
    z_wait(6)
    hidden(6)
    forwards(5)
    z_wait(7)
    hidden(7)
    down(4)
    forwards(6)
    down_early(6)
    down(5)
    mix_gather(1).start()
    forwards(7)
    mix_gather(0).forward()
    down_early(7)
    down(6, True)
    mix_gather(1).forward()
    down(7, True)
    loads[1].wait()

    def mix_project(b):
        mix_gather(b).finish()
        at = slice(b * half_rows, (b + 1) * half_rows)

        @pl.loop(0, dq // out_tile)
        def _(i):
            cols = pl.ds(pl.multiple_of(i * out_tile, out_tile), out_tile)
            out_ref[0, at, cols] = dot(ho[at, :], wo[:, cols]).astype(BF16)

    def taken(ref, sem):
        return pltpu.make_async_copy(ref, ref, sem)

    mix_project(0)
    taken(ret.at[: (ep - 1) * cap, :], r_recv.at[0]).wait()

    @pl.loop(0, dq // out_tile)
    def _(i):
        cols = pl.ds(pl.multiple_of(i * out_tile, out_tile), out_tile)
        came = ret[:, cols]
        out_ref[1, :, cols] = (
            dot(p0[...], came) * narrow[:, 2:3] + dot(p1[...], came) * narrow[:, 3:4]
        ).astype(BF16)

    mix_project(1)

    slim_rows = sum(offsets(u)[1] - offsets(u)[0] for u in range(4)) * cap
    taken(og.at[: ep * cap - cap - slim_rows, :], sent.at[0]).wait()
    taken(og.at[:slim_rows, :dq], sent.at[1]).wait()
    taken(x.at[:slim_rows, : (tp - 1) * dq], sent.at[2]).wait()
    taken(h.at[:, : (tp - 1) * fq], sent.at[3]).wait()
    taken(ho.at[:, : (tp - 1) * heads * hd], sent.at[4]).wait()
    taken(eo.at[: (ep - 1) * cap, :], sent.at[5]).wait()

    @pl.when(core == 0)
    def _():
        up_copy().wait_send()

    @pl.when((core == 1) & (chip < chips - 1))
    def _():
        next_copy().wait_send()

    @pl.when((core == 1) & (chip > 0))
    def _():
        down_copy().wait_send()


def turn_table(ep, rows, hd):
    half = hd // 2
    inverse = np.tile(10000.0 ** (-np.arange(half) / half), 2)
    near = np.arange(rows)[:, None] * inverse[None, :]
    far = (np.arange(ep) * rows)[:, None] * inverse[None, :]
    parts = [np.cos(near), np.sin(near), np.cos(far), np.sin(far)]
    return np.concatenate(parts).astype(np.float32)


def on_device(
    ep, tp,
    queries, keys, values, gates, log_decay, out_weight, moe_rows, moe_gain, routes,
    route_weights, gate_proj, up_proj, down_proj,
):
    rows, d = moe_rows.shape
    heads = log_decay.shape[1]
    width = queries.shape[1]
    hd = width // heads
    cap = 2 * rows // ep
    dq = d // tp
    fq = gate_proj.shape[2]
    ff = down_proj.shape[1]
    slots = 2 if tp == 4 else tp - 1
    units = plan(ep)
    slim = sum(size for low, size, whole in units if not whole) - 2
    blocks = rows // BLOCK
    srows = heads * hd + 8 * ((heads + 7) // 8)
    vmem = pl.BlockSpec(memory_space=pltpu.VMEM)
    dma = pltpu.SemaphoreType.DMA
    table = jnp.asarray(turn_table(ep, rows, hd))
    operands = [
        pltpu.with_memory_space_constraint(operand, pltpu.HBM)
        for operand in (
            queries, keys, values, gates, log_decay.T, table, moe_rows, moe_gain.reshape(-1, 128),
            routes.T, route_weights.T, out_weight, gate_proj, up_proj, down_proj,
        )
    ]
    both = pl.pallas_call(
        functools.partial(kernel, ep, tp),
        out_shape=jax.ShapeDtypeStruct((2, rows, dq), BF16),
        in_specs=[pl.BlockSpec(memory_space=pltpu.HBM)] * 14,
        out_specs=vmem,
        scratch_shapes=[
            pltpu.VMEM((heads, rows), F32),
            pltpu.VMEM((d // 128, 128), BF16),
            pltpu.VMEM((2, rows), jnp.int32),
            pltpu.VMEM((2, rows), F32),
            pltpu.VMEM((4, rows, width), BF16),
            pltpu.VMEM(table.shape, F32),
            pltpu.VMEM((rows, d), BF16),
            pltpu.VMEM((2, rows, hd), F32),
            pltpu.VMEM(out_weight.shape, BF16),
            pltpu.VMEM((d, fq), BF16),
            pltpu.VMEM((d, fq), BF16),
            pltpu.VMEM((ff, dq), BF16),
            pltpu.VMEM((rows, d), BF16),
            pltpu.VMEM((rows, ep * cap), BF16),
            pltpu.VMEM((rows, ep * cap), BF16),
            pltpu.VMEM((ep * cap, d), BF16),
            pltpu.VMEM((ep * cap, d), BF16),
            pltpu.VMEM((ep * cap, ff), BF16),
            pltpu.VMEM((ep * cap, dq), BF16),
            pltpu.VMEM((ep * cap, dq), BF16),
            pltpu.VMEM((rows, width * tp), BF16),
            pltpu.VMEM((2, srows, hd), F32),
            pltpu.VMEM((1, srows, hd), F32),
            pltpu.VMEM((2, heads * hd, hd), BF16),
            pltpu.VMEM((blocks, srows, hd), F32),
            pltpu.VMEM((2, ep // 8 * cap, dq), F32),
            pltpu.VMEM((rows, width), BF16),
            pltpu.VMEM((rows, width), F32),
            pltpu.VMEM((rows, 128), F32),
            pltpu.VMEM((128, rows), F32),
            pltpu.VMEM((rows, 128), F32),
            dma((14,)), dma((6,)), dma((ep,)),
            dma((slim, slots)), dma((slim,)),
            dma((len(units) * 3, slots)), dma((len(units),)),
            dma((1,)),
            dma((2, slots)), dma((2,)),
            dma((3,)), dma((3,)),
        ],
        compiler_params=pltpu.CompilerParams(
            collective_id=0, has_side_effects=True, vmem_limit_bytes=44 * 1024 * 1024
        ),
    )(*operands)
    return both[0], both[1]


def solution(mesh):
    placed = (
        P("ep", "tp"), P("ep", "tp"), P("ep", "tp"), P("ep", "tp"), P("ep", "tp"),
        P(None, "tp"), P("ep", None), P(), P("ep", None), P("ep", None),
        P("ep", None, "tp"), P("ep", None, "tp"), P("ep", None, "tp"),
    )
    return jax.shard_map(
        functools.partial(on_device, mesh.shape["ep"], mesh.shape["tp"]),
        mesh=mesh, in_specs=placed, out_specs=(P("ep", "tp"), P("ep", "tp")), check_vma=False,
    )
```

```python
import functools

import jax
import jax.numpy as jnp
import numpy as np
from jax import lax
from jax.experimental import pallas as pl
from jax.experimental.pallas import tpu as pltpu
from jax.sharding import PartitionSpec as P

BLOCK = 128
MESH = pl.DeviceIdType.MESH
F32 = jnp.float32
BF16 = jnp.bfloat16


def each(low, high, body):
    if high - low <= 8:
        for index in range(low, high):
            body(index)
    else:

        @pl.loop(low, high)
        def _(index):
            body(index)


def span(index, size):
    return pl.ds(pl.multiple_of(index * size, size), size)


def split(value):
    high = value.astype(BF16)
    return high, (value - high.astype(F32)).astype(BF16)


def dot(a, b, dims=((1,), (0,))):
    return lax.dot_general(a, b, (dims, ((), ())), preferred_element_type=F32)


def plan(ep):
    q = ep // 8
    order = ((0, False), (1, False), (4, False), (6, False), (2, True), (5, True), (7, True), (3, True))
    return [(low * q, q, whole) for low, whole in order]


class Gather:
    def __init__(self, tp, region, half, send, recv, hop):
        self.tp, self.region, self.half, self.send = tp, region, half, send
        self.recv, self.hop = recv, hop
        self.me = lax.axis_index("tp")

    def copy(self, ref, recv, to):
        return pltpu.make_async_remote_copy(
            src_ref=ref, dst_ref=ref, send_sem=self.send, recv_sem=recv,
            device_id={"tp": to}, device_id_type=MESH,
        )

    def start(self):
        me, tp = self.me, self.tp
        if tp == 4:
            for k in (1, 2):
                self.copy(self.region(me), self.recv(k - 1), me ^ k).start()
        else:
            for k in range(1, tp):
                self.copy(self.region(me), self.recv(k - 1), lax.rem(me + k, tp)).start()

    def forward(self):
        if self.tp == 4:
            me = self.me
            for k in (1, 2):
                self.copy(self.region(me ^ k), self.recv(k - 1), me ^ k).wait_recv()
                self.copy(self.half(me ^ k, k - 1), self.hop, me ^ (3 - k)).start()

    def finish(self):
        me, tp = self.me, self.tp
        if tp == 4:
            self.copy(self.region(me ^ 3), self.hop, me ^ 3).wait_recv()
        else:
            for k in range(1, tp):
                owner = lax.rem(me + tp - k, tp)
                self.copy(self.region(owner), self.recv(k - 1), owner).wait_recv()


def kernel(
    ep, tp,
    q_hbm, k_hbm, v_hbm, g_hbm, ld_hbm, tab_hbm, rows_hbm, gain_hbm, routes_hbm, rw_hbm,
    wo_hbm, wg_hbm, wu_hbm, wd_hbm,
    out_ref,
    ld_ref, gain_ref, routes_ref, rw_ref, heads_in, tab, rows_ref, turn,
    wo, wg, wu, wd, normed, p0, p1, late0, late1, og, x, h, eo, ret, ret_late, combined, ho, state, landed, passed, excl, partial, mixed,
    rq, inside, cums, pack, narrow,
    w_sem, sent, z_recv, f_recv, f_hop, h_recv, h_hop, r_recv, m_recv, m_hop, s_send, s_recv,
):

    e, t = lax.axis_index("ep"), lax.axis_index("tp")
    rows, d = rows_ref.shape
    cap = 2 * rows // ep
    dq = d // tp
    ff = wd.shape[0]
    fq = ff // tp
    heads = ld_ref.shape[0]
    hd = heads_in.shape[2] // heads
    q_ref, k_ref, v_ref, g_ref = [heads_in.at[i] for i in range(4)]
    blocks = rows // BLOCK
    g = ep // 4
    units = plan(ep)
    tile = min(256, fq)
    pieces = 2 if fq >= 512 else 1
    piece = fq // pieces
    cuts = [(j * piece, piece) for j in range(pieces)]
    first = [(0, tile), (tile, piece - tile)] * (piece > tile) + cuts[piece > tile :]
    core, chip, chips = lax.rem(e, 2), e // 2, ep // 2
    inner = lax.rem(chip + chip // 2, 2) == 1

    barrier = pltpu.get_barrier_semaphore()

    def greet_ep(off):
        pl.semaphore_signal(barrier, inc=1, device_id={"ep": e ^ off}, device_id_type=MESH)

    each(1, ep, greet_ep)
    for k in range(1, tp):
        pl.semaphore_signal(
            barrier, inc=1, device_id={"tp": lax.rem(t + k, tp)}, device_id_type=MESH
        )

    parts = 2
    step_rows = rows // parts
    part_at = [slice(i * step_rows, (i + 1) * step_rows) for i in range(parts)]
    row_loads = [
        pltpu.make_async_copy(rows_hbm.at[at, :], rows_ref.at[at, :], w_sem.at[4 + i])
        for i, at in enumerate(part_at)
    ]
    loads = [
        pltpu.make_async_copy(src, dst, w_sem.at[i])
        for i, (src, dst) in enumerate(
            (
                (wd_hbm.at[0], wd), (wo_hbm, wo), (tab_hbm, tab),
            )
        )
    ]
    head_loads = [
        pltpu.make_async_copy(src, dst, w_sem.at[3])
        for src, dst in ((q_hbm, q_ref), (k_hbm, k_ref), (v_hbm, v_ref), (g_hbm, g_ref))
    ]
    weight_loads = [
        [
            pltpu.make_async_copy(
                src.at[0, :, j * piece : (j + 1) * piece], dst.at[:, j * piece : (j + 1) * piece],
                w_sem.at[6 + 2 * j + i],
            )
            for i, (src, dst) in enumerate(((wg_hbm, wg), (wu_hbm, wu)))
        ]
        for j in range(pieces)
    ]
    small_loads = [
        pltpu.make_async_copy(src, dst, w_sem.at[10 + i])
        for i, (src, dst) in enumerate(
            (
                (routes_hbm, routes_ref), (gain_hbm, gain_ref), (ld_hbm, ld_ref), (rw_hbm, rw_ref),
            )
        )
    ]
    for load in row_loads + small_loads + sum(weight_loads, []):
        load.start()

    small_loads[0].wait()
    routes = [routes_ref[k : k + 1, :] for k in range(2)]
    experts = lax.broadcasted_iota(jnp.int32, (max(8, ep), rows), 0)
    hot = [(experts == routes[k]).astype(F32) for k in range(2)]
    before = (
        lax.broadcasted_iota(jnp.int32, (rows, rows), 0)
        < lax.broadcasted_iota(jnp.int32, (rows, rows), 1)
    ).astype(F32).astype(BF16)
    rank = dot((hot[0] + hot[1]).astype(BF16), before)
    targets = [
        routes[k] * cap + jnp.sum(rank * hot[k], axis=0, keepdims=True).astype(jnp.int32)
        for k in range(2)
    ]

    small_loads[1].wait()
    for i, at in enumerate(part_at):
        row_loads[i].wait()
        squares = None
        for c in range(d // 128):
            val = rows_ref[at, c * 128 : (c + 1) * 128].astype(F32)
            squares = val * val if squares is None else squares + val * val
        scale = lax.rsqrt(jnp.sum(squares, axis=-1, keepdims=True) / d + 1e-06)
        for c in range(d // 128):
            cols = slice(c * 128, (c + 1) * 128)
            val = rows_ref[at, cols].astype(F32)
            normed[at, cols] = (val * scale * gain_ref[c : c + 1, :].astype(F32)).astype(BF16)

    late = (6, 7)

    def group_of(low, size):
        return (e // size) ^ (low // size)

    def unit_at(low, size):
        return span(group_of(low, size), size * cap)

    def pick(low, size):
        slot = lax.broadcasted_iota(jnp.int32, (size * cap, rows), 0) + (
            (e // size) ^ (low // size)
        ) * (size * cap)
        return ((slot == targets[0]) | (slot == targets[1])).astype(F32).astype(BF16)

    def group(low, size, start, width):
        chosen = pick(low, size)
        wide = min(256, width)
        for c in range(width // wide):
            cols = pl.ds(pl.multiple_of(start + c * wide, wide), wide)
            og[unit_at(low, size), cols] = dot(chosen, normed[:, cols]).astype(BF16)

    group(0, g, 0, d)
    for low, size, whole in units[2:4]:
        group(low, size, t * dq, dq)
    pl.semaphore_wait(barrier, ep - 1 + tp - 1)

    def z_copy(off, here, whole):
        other = e ^ off
        land = span(other if here else e, cap)
        if whole:
            src, dst = og.at[span(other, cap), :], x.at[land, :]
        else:
            src, dst = og.at[span(other, cap), span(t, dq)], x.at[land, span(t, dq)]
        return pltpu.make_async_remote_copy(
            src_ref=src, dst_ref=dst, send_sem=sent.at[0 if whole else 1],
            recv_sem=z_recv.at[other if here else e],
            device_id={"ep": other}, device_id_type=MESH,
        )

    def offsets(u):
        low, size, whole = units[u]
        return max(2, low), max(2, low + size), whole

    def z_start(u):
        low, high, whole = offsets(u)
        each(low, high, lambda off: z_copy(off, False, whole).start())

    def z_wait(u):
        low, high, whole = offsets(u)
        each(low, high, lambda off: z_copy(off, True, whole).wait_recv())

    z_copy(1, False, True).start()
    for u in range(4):
        z_start(u)
    for load in head_loads + loads[2:3] + loads[0:2]:
        load.start()
    x[span(e, cap), :] = og[span(e, cap), :]
    group(*units[4][:2], 0, d)
    z_start(4)

    slim_at, count = [], 0
    for u in range(4):
        low, high, _ = offsets(u)
        slim_at.append(count - low)
        count += high - low

    def row_gather(u, off):
        other = e ^ off
        start = other * cap
        at = slim_at[u] + off

        def half(owner, k):
            return x.at[
                pl.ds(pl.multiple_of(start + k * (cap // 2), cap // 2), cap // 2), span(owner, dq)
            ]

        return Gather(
            tp, lambda owner: x.at[span(other, cap), span(owner, dq)], half,
            sent.at[2], lambda slot: f_recv.at[at, slot], f_hop.at[at],
        )

    def rows_start(u):
        low, high, _ = offsets(u)

        def take(off):
            z_copy(off, True, False).wait_recv()
            row_gather(u, off).start()

        each(low, high, take)

    def rows_forward(u):
        low, high, _ = offsets(u)
        each(low, high, lambda off: row_gather(u, off).forward())

    def rows_finish(u):
        low, high, _ = offsets(u)
        each(low, high, lambda off: row_gather(u, off).finish())

    counts = [len(first if u in (0, 4) else cuts) for u in range(len(units))]
    piece_at = [sum(counts[:u]) for u in range(len(units))]

    def hid_gather(u, number):
        start, width = (0, fq) if number is None else (first if u in (0, 4) else cuts)[number]
        low, size, _ = units[u]
        count = size * cap
        base = ((e // size) ^ (low // size)) * count

        def cols(owner):
            return pl.ds(pl.multiple_of(owner * fq + start, tile), width)

        return Gather(
            tp,
            lambda owner: h.at[pl.ds(pl.multiple_of(base, count), count), cols(owner)],
            lambda owner, k: h.at[
                pl.ds(pl.multiple_of(base + k * (count // 2), count // 2), count // 2), cols(owner)
            ],
            sent.at[3], lambda slot: h_recv.at[piece_at[u] + number, slot], h_hop.at[u],
        )

    def hid_finish(u):
        if tp == 4:
            hid_gather(u, None).finish()
        else:
            for j in range(len(first if u in (0, 4) else cuts)):
                hid_gather(u, j).finish()

    half_rows = rows // 2

    def mix_gather(b):
        def at(low, size):
            return slice(b * half_rows + low, b * half_rows + low + size)

        return Gather(
            tp, lambda owner: ho.at[at(0, half_rows), span(owner, heads * hd)],
            lambda owner, k: ho.at[
                at(k * (half_rows // 2), half_rows // 2), span(owner, heads * hd)
            ],
            sent.at[4], lambda slot: m_recv.at[b, slot], m_hop.at[b],
        )

    def hidden_piece(u, j):
        at = unit_at(*units[u][:2])
        start, width = (first if u in (0, 4) else cuts)[j]

        @pl.loop(0, width // tile)
        def _(i):
            cols = pl.ds(pl.multiple_of(start + i * tile, tile), tile)
            held = x[at, :]
            gate = dot(held, wg[:, cols])
            up = dot(held, wu[:, cols])
            hid = (gate / (1.0 + jnp.exp(-gate)) * up).astype(BF16)
            h[at, pl.ds(pl.multiple_of(t * fq + start + i * tile, tile), tile)] = hid

        hid_gather(u, j).start()

    def back_copy(u, off, cols):
        other = e ^ off
        size = units[u][1]
        if u in late:
            row = late.index(u) * size + lax.rem(e, size)
            dst = ret_late.at[pl.ds(pl.multiple_of(row * cap, cap), cap), cols]
        else:
            dst = ret.at[span(e, cap), cols]
        return pltpu.make_async_remote_copy(
            src_ref=eo.at[span(other, cap), cols], dst_ref=dst,
            send_sem=sent.at[5], recv_sem=r_recv.at[1 if u in late else 0],
            device_id={"ep": other}, device_id_type=MESH,
        )

    out_tile = min(256, dq)

    def mix_early(b):
        if tp == 4:
            at = slice(b * half_rows, (b + 1) * half_rows)
            share = heads * hd

            @pl.loop(0, dq // out_tile)
            def _(i):
                cols = pl.ds(pl.multiple_of(i * out_tile, out_tile), out_tile)
                mixed[at, cols] = sum(
                    dot(ho[at, span(t ^ k, share)], wo[span(t ^ k, share), cols]) for k in range(3)
                )

    def mix_project(b):
        mix_gather(b).finish()
        at = slice(b * half_rows, (b + 1) * half_rows)
        share = heads * hd

        @pl.loop(0, dq // out_tile)
        def _(i):
            cols = pl.ds(pl.multiple_of(i * out_tile, out_tile), out_tile)
            if tp == 4:
                total = mixed[at, cols] + dot(
                    ho[at, span(t ^ 3, share)], wo[span(t ^ 3, share), cols]
                )
            else:
                total = dot(ho[at, :], wo[:, cols])
            out_ref[0, at, cols] = total.astype(BF16)

    def down_early(u):
        if tp == 4:
            at = unit_at(*units[u][:2])

            @pl.loop(0, dq // out_tile)
            def _(i):
                cols = pl.ds(pl.multiple_of(i * out_tile, out_tile), out_tile)
                partial[u % 2, :, cols] = sum(
                    dot(h[at, span(t ^ k, fq)], wd[span(t ^ k, fq), cols]) for k in range(3)
                )

    def down(u, early=False):
        hid_finish(u)
        low, size, _ = units[u]
        at = unit_at(low, size)

        @pl.loop(0, dq // out_tile)
        def _(i):
            cols = pl.ds(pl.multiple_of(i * out_tile, out_tile), out_tile)
            if early and tp == 4:
                done = t ^ 3
                total = partial[u % 2, :, cols] + dot(
                    h[at, span(done, fq)], wd[span(done, fq), cols]
                )
            else:
                total = dot(h[at, :], wd[:, cols])
            eo[at, cols] = total.astype(BF16)
            each(max(1, low), low + size, lambda off: back_copy(u, off, cols).start())

        if low == 0:
            ret[span(e, cap), :] = eo[span(e, cap), :]

    def forward(u, j):
        hid_gather(u, j).forward()

    row_i = lax.broadcasted_iota(jnp.int32, (BLOCK, BLOCK), 0)
    col_j = lax.broadcasted_iota(jnp.int32, (BLOCK, BLOCK), 1)
    causal = row_i >= col_j
    lower = causal.astype(F32)
    factor = hd ** (-0.5)
    decay_at = heads * hd

    def retention_local():
        small_loads[2].wait()
        small_loads[3].wait()
        pack[...] = jnp.zeros_like(pack)
        pack[0:1, :] = targets[0].astype(F32)
        pack[1:2, :] = targets[1].astype(F32)
        pack[2:4, :] = rw_ref[...]
        pack[4 : 4 + heads, :] = ld_ref[...]
        for b in range(rows // 128):
            narrow[b * 128 : (b + 1) * 128, :] = pack[:, b * 128 : (b + 1) * 128].T
        lanes = lax.broadcasted_iota(jnp.int32, (rows, ep * cap), 1)
        for k, ref in ((0, p0), (1, p1)):
            ref[...] = (lanes == narrow[:, k : k + 1].astype(jnp.int32)).astype(F32).astype(BF16)
        count = units[late[0]][1] * cap
        place = lax.broadcasted_iota(jnp.int32, (rows, 2 * count), 1)
        bases = [group_of(*units[u][:2]) * count for u in late]
        slot = jnp.where(place < count, place + bases[0], place - count + bases[1])
        for k, ref in ((0, late0), (1, late1)):
            ref[...] = (slot == narrow[:, k : k + 1].astype(jnp.int32)).astype(F32).astype(BF16)
        for u in late:
            ret[unit_at(*units[u][:2]), :] = jnp.zeros((count, dq), BF16)
        loads[2].wait()
        pltpu.make_async_copy(heads_in, heads_in, w_sem.at[3]).wait()
        here_cos = tab[pl.ds(2 * rows + e, 1), :]
        here_sin = tab[pl.ds(2 * rows + ep + e, 1), :]
        sign = jnp.where(lax.broadcasted_iota(jnp.int32, (BLOCK, hd), 1) < hd // 2, -1.0, 1.0)
        for b in range(blocks):
            at = slice(b * BLOCK, (b + 1) * BLOCK)
            cos, sin = tab[at, :], tab[slice(rows + b * BLOCK, rows + (b + 1) * BLOCK), :]
            turn[0, at, :] = cos * here_cos - sin * here_sin
            turn[1, at, :] = (sin * here_cos + cos * here_sin) * sign
            cums[at, :] = lax.dot_general(
                lower, narrow[at, :], (((1,), (0,)), ((), ())),
                preferred_element_type=F32, precision=lax.Precision.HIGHEST,
            )
        for n in range(heads):
            cols = slice(n * hd, (n + 1) * hd)
            total = None
            gone = None
            for b in range(blocks):
                at = slice(b * BLOCK, (b + 1) * BLOCK)
                cos, sin = turn[0, at, :], turn[1, at, :]

                def turned(ref):
                    val = ref[at, cols].astype(F32)
                    return val * cos + pltpu.roll(val, hd // 2, 1) * sin

                qb = turned(q_ref).astype(BF16)
                kb = (turned(k_ref) * factor).astype(BF16)
                vb = v_ref[at, cols]
                rq[at, cols] = qb
                cum = jnp.broadcast_to(cums[at, 4 + n : 5 + n], (BLOCK, BLOCK))
                spread = cum - cum.T
                weight = jnp.where(causal, jnp.exp(jnp.where(causal, spread, 0.0)), 0.0)
                scores = dot(qb, kb, ((1,), (1,)))
                inside[at, cols] = dot((scores * weight).astype(BF16), vb)
                ending = cum[BLOCK - 1 : BLOCK, :]
                k_hi, k_lo = split(kb.astype(F32) * jnp.exp(ending - cum))
                update = dot(k_hi, vb, ((0,), (0,))) + dot(k_lo, vb, ((0,), (0,)))
                if b == 0:
                    total, gone = update, ending
                else:
                    total = jnp.exp(ending) * total + update
                    gone = gone + ending
                if b < blocks - 1:
                    excl[1 + b, n * hd : (n + 1) * hd, :] = total
            state[0, n * hd : (n + 1) * hd, :] = total
            state[0, decay_at + n : decay_at + n + 1, :] = jnp.exp(gone)
        excl[0, :decay_at, :] = jnp.zeros((decay_at, hd), F32)

    def up_copy():
        return pltpu.make_async_remote_copy(
            src_ref=state.at[0], dst_ref=landed.at[0], send_sem=s_send.at[0],
            recv_sem=s_recv.at[0], device_id={"ep": e ^ 1}, device_id_type=MESH,
        )

    def next_copy():
        return pltpu.make_async_remote_copy(
            src_ref=passed.at[0], dst_ref=passed.at[1],
            send_sem=s_send.at[1], recv_sem=s_recv.at[1],
            device_id={"ep": lax.rem(e + 2, ep)}, device_id_type=MESH,
        )

    def down_copy():
        return pltpu.make_async_remote_copy(
            src_ref=passed.at[1], dst_ref=passed.at[1], send_sem=s_send.at[2], recv_sem=s_recv.at[2],
            device_id={"ep": e ^ 1}, device_id_type=MESH,
        )

    def decays(n):
        at = slice(decay_at + n, decay_at + n + 1)
        return landed[0, at, :], state[0, at, :]

    def scan_open():
        @pl.when(core == 1)
        def _():
            up_copy().wait_recv()
            for n in range(heads):
                at = slice(n * hd, (n + 1) * hd)
                mine = decays(n)[1]
                state[1, at, :] = mine * landed[0, at, :] + state[0, at, :]
                excl[0, at, :] = landed[0, at, :]
            passed[0] = state[1, :decay_at, :].astype(BF16)

        if chips > 1:

            @pl.when((core == 1) & (chip == 0))
            def _():
                next_copy().start()

    def scan_pass(turn_of):
        @pl.when((core == 1) & turn_of)
        def _():
            next_copy().wait_recv()
            down_copy().start()
            for n in range(heads):
                at = slice(n * hd, (n + 1) * hd)
                first, mine = decays(n)
                came = passed[1, at, :].astype(F32)
                passed[0, at, :] = ((first * mine) * came + state[1, at, :]).astype(BF16)
                excl[0, at, :] = first * came + excl[0, at, :]

        @pl.when((core == 1) & turn_of & (chip < chips - 1))
        def _():
            next_copy().start()

    def scan_close():
        @pl.when((core == 0) & (chip > 0))
        def _():
            down_copy().wait_recv()
            excl[0, :decay_at, :] = passed[1].astype(F32)

    def retention_close():
        for n in range(heads):
            cols = slice(n * hd, (n + 1) * hd)
            sat = slice(n * hd, (n + 1) * hd)
            entering = excl[0, sat, :]
            gone = None
            for b in range(blocks):
                at = slice(b * BLOCK, (b + 1) * BLOCK)
                cum = jnp.broadcast_to(cums[at, 4 + n : 5 + n], (BLOCK, hd))
                held = entering if b == 0 else jnp.exp(gone) * entering + excl[b, sat, :]
                hi, lo = split(held)
                qb = rq[at, cols]
                retained = inside[at, cols] + (dot(qb, hi) + dot(qb, lo)) * jnp.exp(cum)
                scale = lax.rsqrt(jnp.mean(retained * retained, axis=-1, keepdims=True) + 1e-05)
                gate = g_ref[at, cols].astype(F32)
                out = (retained * scale * (gate / (1.0 + jnp.exp(-gate)))).astype(BF16)
                ho[at, pl.ds(pl.multiple_of(t * heads * hd + n * hd, hd), hd)] = out
                ending = cum[BLOCK - 1 : BLOCK, :]
                gone = ending if gone is None else gone + ending

    for load in weight_loads[0]:
        load.wait()

    def take_partner(u):
        if units[u][0] <= 1 < units[u][0] + units[u][1]:
            z_copy(1, True, True).wait_recv()
        rows_start(u)
        rows_forward(u)
        rows_finish(u)

    def hidden(u):
        for j in range(len(first if u in (0, 4) else cuts)):
            hidden_piece(u, j)

    def forwards(u):
        for j in range(len(first if u in (0, 4) else cuts)):
            forward(u, j)

    take_partner(0)
    for j in range(len(first) - pieces + 1):
        hidden_piece(0, j)
    for j in range(1, pieces):
        for load in weight_loads[j]:
            load.wait()
        hidden_piece(0, j + len(first) - pieces)
    take_partner(1)
    hidden_piece(1, 0)
    retention_local()

    @pl.when(core == 0)
    def _():
        up_copy().start()

    for j in range(len(first) - 1):
        forward(0, j)
    for low, size, whole in units[5:]:
        group(low, size, 0, d)


    early = jnp.logical_not(inner) & (core == 0)

    @pl.when(early)
    def _():
        z_start(5)

    forward(0, len(first) - 1)
    rows_start(2)
    for j in range(1, pieces):
        hidden_piece(1, j)
    scan_open()

    rows_start(3)

    @pl.when(jnp.logical_not(early))
    def _():
        z_start(5)

    @pl.when(core == 0)
    def _():
        z_start(6)

    forward(1, 0)
    rows_forward(2)
    for j in range(1, pieces):
        forward(1, j)
    z_wait(4)
    hidden(4)
    scan_pass(chip == 1)

    @pl.when(core == 1)
    def _():
        z_start(6)

    rows_forward(3)
    rows_finish(2)
    hidden(2)
    forwards(4)
    rows_finish(3)
    hidden(3)

    @pl.when(core == 0)
    def _():
        z_start(7)

    loads[0].wait()
    down(0)
    forwards(2)
    z_wait(5)
    for j in range(pieces):
        hidden_piece(5, j)
        forward(3, j)
    scan_pass(chip == 2)

    @pl.when(core == 1)
    def _():
        z_start(7)

    down(1)
    scan_pass(chip > 2)
    scan_close()
    retention_close()
    mix_gather(0).start()
    down(4)
    z_wait(6)
    hidden(6)
    forwards(5)
    down(2)
    z_wait(7)
    hidden(7)
    down(3)
    forwards(6)
    down_early(6)
    down(5)
    mix_gather(1).start()
    forwards(7)
    mix_gather(0).forward()
    down_early(7)
    down(6, True)
    loads[1].wait()
    mix_early(0)
    mix_gather(1).forward()
    mix_early(1)

    def taken(ref, sem):
        return pltpu.make_async_copy(ref, ref, sem)

    def weighed(first_pick, second_pick, came):
        return (
            dot(first_pick[...], came) * narrow[:, 2:3]
            + dot(second_pick[...], came) * narrow[:, 3:4]
        )

    taken(ret.at[: (ep - 1) * cap - ret_late.shape[0], :], r_recv.at[0]).wait()

    @pl.loop(0, dq // out_tile)
    def _(i):
        cols = pl.ds(pl.multiple_of(i * out_tile, out_tile), out_tile)
        combined[:, cols] = weighed(p0, p1, ret[:, cols])

    down(7, True)
    mix_project(0)
    mix_project(1)
    taken(ret_late, r_recv.at[1]).wait()

    @pl.loop(0, dq // out_tile)
    def _(i):
        cols = pl.ds(pl.multiple_of(i * out_tile, out_tile), out_tile)
        out_ref[1, :, cols] = (
            combined[:, cols] + weighed(late0, late1, ret_late[:, cols])
        ).astype(BF16)

    slim_rows = sum(offsets(u)[1] - offsets(u)[0] for u in range(4)) * cap
    taken(og.at[: ep * cap - cap - slim_rows, :], sent.at[0]).wait()
    taken(og.at[:slim_rows, :dq], sent.at[1]).wait()
    taken(x.at[:slim_rows, : (tp - 1) * dq], sent.at[2]).wait()
    taken(h.at[:, : (tp - 1) * fq], sent.at[3]).wait()
    taken(ho.at[:, : (tp - 1) * heads * hd], sent.at[4]).wait()
    taken(eo.at[: (ep - 1) * cap, :], sent.at[5]).wait()

    @pl.when(core == 0)
    def _():
        up_copy().wait_send()

    @pl.when((core == 1) & (chip < chips - 1))
    def _():
        next_copy().wait_send()

    @pl.when((core == 1) & (chip > 0))
    def _():
        down_copy().wait_send()


def turn_table(ep, rows, hd):
    half = hd // 2
    inverse = np.tile(10000.0 ** (-np.arange(half) / half), 2)
    near = np.arange(rows)[:, None] * inverse[None, :]
    far = (np.arange(ep) * rows)[:, None] * inverse[None, :]
    parts = [np.cos(near), np.sin(near), np.cos(far), np.sin(far)]
    return np.concatenate(parts).astype(np.float32)


def on_device(
    ep, tp,
    queries, keys, values, gates, log_decay, out_weight, moe_rows, moe_gain, routes,
    route_weights, gate_proj, up_proj, down_proj,
):
    rows, d = moe_rows.shape
    heads = log_decay.shape[1]
    width = queries.shape[1]
    hd = width // heads
    cap = 2 * rows // ep
    dq = d // tp
    fq = gate_proj.shape[2]
    ff = down_proj.shape[1]
    slots = 2 if tp == 4 else tp - 1
    units = plan(ep)
    slim = sum(size for low, size, whole in units if not whole) - 2
    blocks = rows // BLOCK
    srows = heads * hd + 8 * ((heads + 7) // 8)
    vmem = pl.BlockSpec(memory_space=pltpu.VMEM)
    dma = pltpu.SemaphoreType.DMA
    table = jnp.asarray(turn_table(ep, rows, hd))
    operands = [
        pltpu.with_memory_space_constraint(operand, pltpu.HBM)
        for operand in (
            queries, keys, values, gates, log_decay.T, table, moe_rows, moe_gain.reshape(-1, 128),
            routes.T, route_weights.T, out_weight, gate_proj, up_proj, down_proj,
        )
    ]
    both = pl.pallas_call(
        functools.partial(kernel, ep, tp),
        out_shape=jax.ShapeDtypeStruct((2, rows, dq), BF16),
        in_specs=[pl.BlockSpec(memory_space=pltpu.HBM)] * 14,
        out_specs=vmem,
        scratch_shapes=[
            pltpu.VMEM((heads, rows), F32),
            pltpu.VMEM((d // 128, 128), BF16),
            pltpu.VMEM((2, rows), jnp.int32),
            pltpu.VMEM((2, rows), F32),
            pltpu.VMEM((4, rows, width), BF16),
            pltpu.VMEM(table.shape, F32),
            pltpu.VMEM((rows, d), BF16),
            pltpu.VMEM((2, rows, hd), F32),
            pltpu.VMEM(out_weight.shape, BF16),
            pltpu.VMEM((d, fq), BF16),
            pltpu.VMEM((d, fq), BF16),
            pltpu.VMEM((ff, dq), BF16),
            pltpu.VMEM((rows, d), BF16),
            pltpu.VMEM((rows, ep * cap), BF16),
            pltpu.VMEM((rows, ep * cap), BF16),
            pltpu.VMEM((rows, ep // 4 * cap), BF16),
            pltpu.VMEM((rows, ep // 4 * cap), BF16),
            pltpu.VMEM((ep * cap, d), BF16),
            pltpu.VMEM((ep * cap, d), BF16),
            pltpu.VMEM((ep * cap, ff), BF16),
            pltpu.VMEM((ep * cap, dq), BF16),
            pltpu.VMEM((ep * cap, dq), BF16),
            pltpu.VMEM((ep // 4 * cap, dq), BF16),
            pltpu.VMEM((rows, dq), F32),
            pltpu.VMEM((rows, width * tp), BF16),
            pltpu.VMEM((2, srows, hd), F32),
            pltpu.VMEM((1, srows, hd), F32),
            pltpu.VMEM((2, heads * hd, hd), BF16),
            pltpu.VMEM((blocks, srows, hd), F32),
            pltpu.VMEM((2, ep // 8 * cap, dq), F32),
            pltpu.VMEM((rows, dq), F32),
            pltpu.VMEM((rows, width), BF16),
            pltpu.VMEM((rows, width), F32),
            pltpu.VMEM((rows, 128), F32),
            pltpu.VMEM((128, rows), F32),
            pltpu.VMEM((rows, 128), F32),
            dma((14,)), dma((6,)), dma((ep,)),
            dma((slim, slots)), dma((slim,)),
            dma((len(units) * 2 + 2, slots)), dma((len(units),)),
            dma((2,)),
            dma((2, slots)), dma((2,)),
            dma((3,)), dma((3,)),
        ],
        compiler_params=pltpu.CompilerParams(
            collective_id=0, has_side_effects=True, vmem_limit_bytes=44 * 1024 * 1024
        ),
    )(*operands)
    return both[0], both[1]


def solution(mesh):
    placed = (
        P("ep", "tp"), P("ep", "tp"), P("ep", "tp"), P("ep", "tp"), P("ep", "tp"),
        P(None, "tp"), P("ep", None), P(), P("ep", None), P("ep", None),
        P("ep", None, "tp"), P("ep", None, "tp"), P("ep", None, "tp"),
    )
    return jax.shard_map(
        functools.partial(on_device, mesh.shape["ep"], mesh.shape["tp"]),
        mesh=mesh, in_specs=placed, out_specs=(P("ep", "tp"), P("ep", "tp")), check_vma=False,
    )
```

```python
import functools

import jax
import jax.numpy as jnp
import numpy as np
from jax import lax
from jax.experimental import pallas as pl
from jax.experimental.pallas import tpu as pltpu
from jax.sharding import PartitionSpec as P

BLOCK = 128
MESH = pl.DeviceIdType.MESH
F32 = jnp.float32
BF16 = jnp.bfloat16


def each(low, high, body):
    if high - low <= 8:
        for index in range(low, high):
            body(index)
    else:

        @pl.loop(low, high)
        def _(index):
            body(index)


def span(index, size):
    return pl.ds(pl.multiple_of(index * size, size), size)


def split(value):
    high = value.astype(BF16)
    return high, (value - high.astype(F32)).astype(BF16)


def dot(a, b, dims=((1,), (0,))):
    return lax.dot_general(a, b, (dims, ((), ())), preferred_element_type=F32)


def plan(ep):
    q = ep // 8
    order = ((0, False), (1, False), (4, False), (6, False), (2, True), (5, True), (7, True), (3, True))
    return [(low * q, q, whole) for low, whole in order]


class Gather:
    def __init__(self, tp, region, half, send, recv, hop):
        self.tp, self.region, self.half, self.send = tp, region, half, send
        self.recv, self.hop = recv, hop
        self.me = lax.axis_index("tp")

    def copy(self, ref, recv, to):
        return pltpu.make_async_remote_copy(
            src_ref=ref, dst_ref=ref, send_sem=self.send, recv_sem=recv,
            device_id={"tp": to}, device_id_type=MESH,
        )

    def start(self):
        me, tp = self.me, self.tp
        if tp == 4:
            for k in (1, 2):
                self.copy(self.region(me), self.recv(k - 1), me ^ k).start()
        else:
            for k in range(1, tp):
                self.copy(self.region(me), self.recv(k - 1), lax.rem(me + k, tp)).start()

    def forward(self):
        if self.tp == 4:
            me = self.me
            for k in (1, 2):
                self.copy(self.region(me ^ k), self.recv(k - 1), me ^ k).wait_recv()
                self.copy(self.half(me ^ k, k - 1), self.hop, me ^ (3 - k)).start()

    def finish(self):
        me, tp = self.me, self.tp
        if tp == 4:
            self.copy(self.region(me ^ 3), self.hop, me ^ 3).wait_recv()
        else:
            for k in range(1, tp):
                owner = lax.rem(me + tp - k, tp)
                self.copy(self.region(owner), self.recv(k - 1), owner).wait_recv()


def kernel(
    ep, tp,
    q_hbm, k_hbm, v_hbm, g_hbm, ld_hbm, tab_hbm, rows_hbm, gain_hbm, routes_hbm, rw_hbm,
    wo_hbm, wg_hbm, wu_hbm, wd_hbm,
    out_ref,
    ld_ref, gain_ref, routes_ref, rw_ref, heads_in, tab, rows_ref, turn,
    wo, wg, wu, wd, normed, p0, p1, late0, late1, og, x, h, eo, ret, ret_late, combined, ho, state, landed, passed, excl, partial, mixed,
    rq, inside, cums, pack, narrow,
    w_sem, sent, z_recv, f_recv, f_hop, h_recv, h_hop, r_recv, m_recv, m_hop, s_send, s_recv,
):

    e, t = lax.axis_index("ep"), lax.axis_index("tp")
    rows, d = rows_ref.shape
    cap = 2 * rows // ep
    dq = d // tp
    ff = wd.shape[0]
    fq = ff // tp
    heads = ld_ref.shape[0]
    hd = heads_in.shape[2] // heads
    q_ref, k_ref, v_ref, g_ref = [heads_in.at[i] for i in range(4)]
    blocks = rows // BLOCK
    g = ep // 4
    units = plan(ep)
    tile = min(256, fq)
    pieces = 2 if fq >= 512 else 1
    piece = fq // pieces
    cuts = [(j * piece, piece) for j in range(pieces)]
    first = [(0, tile), (tile, piece - tile)] * (piece > tile) + cuts[piece > tile :]
    core, chip, chips = lax.rem(e, 2), e // 2, ep // 2
    inner = lax.rem(chip + chip // 2, 2) == 1

    barrier = pltpu.get_barrier_semaphore()

    def greet_ep(off):
        pl.semaphore_signal(barrier, inc=1, device_id={"ep": e ^ off}, device_id_type=MESH)

    each(1, ep, greet_ep)
    for k in range(1, tp):
        pl.semaphore_signal(
            barrier, inc=1, device_id={"tp": lax.rem(t + k, tp)}, device_id_type=MESH
        )

    parts = 2
    step_rows = rows // parts
    part_at = [slice(i * step_rows, (i + 1) * step_rows) for i in range(parts)]
    row_loads = [
        pltpu.make_async_copy(rows_hbm.at[at, :], rows_ref.at[at, :], w_sem.at[4 + i])
        for i, at in enumerate(part_at)
    ]
    loads = [
        pltpu.make_async_copy(src, dst, w_sem.at[i])
        for i, (src, dst) in enumerate(
            (
                (wd_hbm.at[0], wd), (wo_hbm, wo), (tab_hbm, tab),
            )
        )
    ]
    head_loads = [
        pltpu.make_async_copy(src, dst, w_sem.at[3])
        for src, dst in ((q_hbm, q_ref), (k_hbm, k_ref), (v_hbm, v_ref), (g_hbm, g_ref))
    ]
    weight_loads = [
        [
            pltpu.make_async_copy(
                src.at[0, :, j * piece : (j + 1) * piece], dst.at[:, j * piece : (j + 1) * piece],
                w_sem.at[6 + 2 * j + i],
            )
            for i, (src, dst) in enumerate(((wg_hbm, wg), (wu_hbm, wu)))
        ]
        for j in range(pieces)
    ]
    small_loads = [
        pltpu.make_async_copy(src, dst, w_sem.at[10 + i])
        for i, (src, dst) in enumerate(
            (
                (routes_hbm, routes_ref), (gain_hbm, gain_ref), (ld_hbm, ld_ref), (rw_hbm, rw_ref),
            )
        )
    ]
    for load in row_loads + small_loads + sum(weight_loads, []):
        load.start()

    small_loads[0].wait()
    routes = [routes_ref[k : k + 1, :] for k in range(2)]
    experts = lax.broadcasted_iota(jnp.int32, (max(8, ep), rows), 0)
    hot = [(experts == routes[k]).astype(F32) for k in range(2)]
    before = (
        lax.broadcasted_iota(jnp.int32, (rows, rows), 0)
        < lax.broadcasted_iota(jnp.int32, (rows, rows), 1)
    ).astype(F32).astype(BF16)
    rank = dot((hot[0] + hot[1]).astype(BF16), before)
    targets = [
        routes[k] * cap + jnp.sum(rank * hot[k], axis=0, keepdims=True).astype(jnp.int32)
        for k in range(2)
    ]

    small_loads[1].wait()
    for i, at in enumerate(part_at):
        row_loads[i].wait()
        squares = None
        for c in range(d // 128):
            val = rows_ref[at, c * 128 : (c + 1) * 128].astype(F32)
            squares = val * val if squares is None else squares + val * val
        scale = lax.rsqrt(jnp.sum(squares, axis=-1, keepdims=True) / d + 1e-06)
        for c in range(d // 128):
            cols = slice(c * 128, (c + 1) * 128)
            val = rows_ref[at, cols].astype(F32)
            normed[at, cols] = (val * scale * gain_ref[c : c + 1, :].astype(F32)).astype(BF16)

    late = (6, 7)

    def group_of(low, size):
        return (e // size) ^ (low // size)

    def unit_at(low, size):
        return span(group_of(low, size), size * cap)

    def pick(low, size):
        slot = lax.broadcasted_iota(jnp.int32, (size * cap, rows), 0) + (
            (e // size) ^ (low // size)
        ) * (size * cap)
        return ((slot == targets[0]) | (slot == targets[1])).astype(F32).astype(BF16)

    def group(low, size, start, width):
        chosen = pick(low, size)
        wide = min(256, width)
        for c in range(width // wide):
            cols = pl.ds(pl.multiple_of(start + c * wide, wide), wide)
            og[unit_at(low, size), cols] = dot(chosen, normed[:, cols]).astype(BF16)

    group(0, g, 0, d)
    for low, size, whole in units[2:4]:
        group(low, size, t * dq, dq)
    pl.semaphore_wait(barrier, ep - 1 + tp - 1)

    def z_copy(off, here, whole):
        other = e ^ off
        land = span(other if here else e, cap)
        if whole:
            src, dst = og.at[span(other, cap), :], x.at[land, :]
        else:
            src, dst = og.at[span(other, cap), span(t, dq)], x.at[land, span(t, dq)]
        return pltpu.make_async_remote_copy(
            src_ref=src, dst_ref=dst, send_sem=sent.at[0 if whole else 1],
            recv_sem=z_recv.at[other if here else e],
            device_id={"ep": other}, device_id_type=MESH,
        )

    def offsets(u):
        low, size, whole = units[u]
        return max(2, low), max(2, low + size), whole

    def z_start(u):
        low, high, whole = offsets(u)
        each(low, high, lambda off: z_copy(off, False, whole).start())

    def z_wait(u):
        low, high, whole = offsets(u)
        each(low, high, lambda off: z_copy(off, True, whole).wait_recv())

    z_copy(1, False, True).start()
    for u in range(4):
        z_start(u)
    for load in head_loads + loads[2:3] + loads[0:2]:
        load.start()
    x[span(e, cap), :] = og[span(e, cap), :]
    group(*units[4][:2], 0, d)
    z_start(4)

    slim_at, count = [], 0
    for u in range(4):
        low, high, _ = offsets(u)
        slim_at.append(count - low)
        count += high - low

    def row_gather(u, off):
        other = e ^ off
        start = other * cap
        at = slim_at[u] + off

        def half(owner, k):
            return x.at[
                pl.ds(pl.multiple_of(start + k * (cap // 2), cap // 2), cap // 2), span(owner, dq)
            ]

        return Gather(
            tp, lambda owner: x.at[span(other, cap), span(owner, dq)], half,
            sent.at[2], lambda slot: f_recv.at[at, slot], f_hop.at[at],
        )

    def rows_start(u):
        low, high, _ = offsets(u)

        def take(off):
            z_copy(off, True, False).wait_recv()
            row_gather(u, off).start()

        each(low, high, take)

    def rows_forward(u):
        low, high, _ = offsets(u)
        each(low, high, lambda off: row_gather(u, off).forward())

    def rows_finish(u):
        low, high, _ = offsets(u)
        each(low, high, lambda off: row_gather(u, off).finish())

    counts = [len(first if u in (0, 4) else cuts) for u in range(len(units))]
    piece_at = [sum(counts[:u]) for u in range(len(units))]

    def hid_gather(u, number):
        start, width = (0, fq) if number is None else (first if u in (0, 4) else cuts)[number]
        low, size, _ = units[u]
        count = size * cap
        base = ((e // size) ^ (low // size)) * count

        def cols(owner):
            return pl.ds(pl.multiple_of(owner * fq + start, tile), width)

        return Gather(
            tp,
            lambda owner: h.at[pl.ds(pl.multiple_of(base, count), count), cols(owner)],
            lambda owner, k: h.at[
                pl.ds(pl.multiple_of(base + k * (count // 2), count // 2), count // 2), cols(owner)
            ],
            sent.at[3], lambda slot: h_recv.at[piece_at[u] + number, slot], h_hop.at[u],
        )

    def hid_finish(u):
        if tp == 4:
            hid_gather(u, None).finish()
        else:
            for j in range(len(first if u in (0, 4) else cuts)):
                hid_gather(u, j).finish()

    half_rows = rows // 2

    def mix_gather(b):
        def at(low, size):
            return slice(b * half_rows + low, b * half_rows + low + size)

        return Gather(
            tp, lambda owner: ho.at[at(0, half_rows), span(owner, heads * hd)],
            lambda owner, k: ho.at[
                at(k * (half_rows // 2), half_rows // 2), span(owner, heads * hd)
            ],
            sent.at[4], lambda slot: m_recv.at[b, slot], m_hop.at[b],
        )

    def hidden_piece(u, j):
        at = unit_at(*units[u][:2])
        start, width = (first if u in (0, 4) else cuts)[j]

        @pl.loop(0, width // tile)
        def _(i):
            cols = pl.ds(pl.multiple_of(start + i * tile, tile), tile)
            held = x[at, :]
            gate = dot(held, wg[:, cols])
            up = dot(held, wu[:, cols])
            hid = (gate / (1.0 + jnp.exp(-gate)) * up).astype(BF16)
            h[at, pl.ds(pl.multiple_of(t * fq + start + i * tile, tile), tile)] = hid

        hid_gather(u, j).start()

    def back_copy(u, off, cols):
        other = e ^ off
        size = units[u][1]
        if u in late:
            row = late.index(u) * size + lax.rem(e, size)
            dst = ret_late.at[pl.ds(pl.multiple_of(row * cap, cap), cap), cols]
        else:
            dst = ret.at[span(e, cap), cols]
        return pltpu.make_async_remote_copy(
            src_ref=eo.at[span(other, cap), cols], dst_ref=dst,
            send_sem=sent.at[5], recv_sem=r_recv.at[1 if u in late else 0],
            device_id={"ep": other}, device_id_type=MESH,
        )

    out_tile = min(256, dq)

    def mix_early(b):
        if tp == 4:
            at = slice(b * half_rows, (b + 1) * half_rows)
            share = heads * hd

            @pl.loop(0, dq // out_tile)
            def _(i):
                cols = pl.ds(pl.multiple_of(i * out_tile, out_tile), out_tile)
                mixed[at, cols] = sum(
                    dot(ho[at, span(t ^ k, share)], wo[span(t ^ k, share), cols]) for k in range(3)
                )

    def mix_project(b):
        mix_gather(b).finish()
        at = slice(b * half_rows, (b + 1) * half_rows)
        share = heads * hd

        @pl.loop(0, dq // out_tile)
        def _(i):
            cols = pl.ds(pl.multiple_of(i * out_tile, out_tile), out_tile)
            if tp == 4:
                total = mixed[at, cols] + dot(
                    ho[at, span(t ^ 3, share)], wo[span(t ^ 3, share), cols]
                )
            else:
                total = dot(ho[at, :], wo[:, cols])
            out_ref[0, at, cols] = total.astype(BF16)

    def down_early(u):
        if tp == 4:
            at = unit_at(*units[u][:2])

            @pl.loop(0, dq // out_tile)
            def _(i):
                cols = pl.ds(pl.multiple_of(i * out_tile, out_tile), out_tile)
                partial[u % 2, :, cols] = sum(
                    dot(h[at, span(t ^ k, fq)], wd[span(t ^ k, fq), cols]) for k in range(3)
                )

    def down(u, early=False):
        hid_finish(u)
        low, size, _ = units[u]
        at = unit_at(low, size)

        @pl.loop(0, dq // out_tile)
        def _(i):
            cols = pl.ds(pl.multiple_of(i * out_tile, out_tile), out_tile)
            if early and tp == 4:
                done = t ^ 3
                total = partial[u % 2, :, cols] + dot(
                    h[at, span(done, fq)], wd[span(done, fq), cols]
                )
            else:
                total = dot(h[at, :], wd[:, cols])
            eo[at, cols] = total.astype(BF16)
            each(max(1, low), low + size, lambda off: back_copy(u, off, cols).start())

        if low == 0:
            ret[span(e, cap), :] = eo[span(e, cap), :]

    def forward(u, j):
        hid_gather(u, j).forward()

    row_i = lax.broadcasted_iota(jnp.int32, (BLOCK, BLOCK), 0)
    col_j = lax.broadcasted_iota(jnp.int32, (BLOCK, BLOCK), 1)
    causal = row_i >= col_j
    lower = causal.astype(F32)
    factor = hd ** (-0.5)
    decay_at = heads * hd

    def retention_local():
        small_loads[2].wait()
        small_loads[3].wait()
        pack[...] = jnp.zeros_like(pack)
        pack[0:1, :] = targets[0].astype(F32)
        pack[1:2, :] = targets[1].astype(F32)
        pack[2:4, :] = rw_ref[...]
        pack[4 : 4 + heads, :] = ld_ref[...]
        for b in range(rows // 128):
            narrow[b * 128 : (b + 1) * 128, :] = pack[:, b * 128 : (b + 1) * 128].T
        lanes = lax.broadcasted_iota(jnp.int32, (rows, ep * cap), 1)
        for k, ref in ((0, p0), (1, p1)):
            ref[...] = (lanes == narrow[:, k : k + 1].astype(jnp.int32)).astype(F32).astype(BF16)
        count = units[late[0]][1] * cap
        place = lax.broadcasted_iota(jnp.int32, (rows, 2 * count), 1)
        bases = [group_of(*units[u][:2]) * count for u in late]
        slot = jnp.where(place < count, place + bases[0], place - count + bases[1])
        for k, ref in ((0, late0), (1, late1)):
            ref[...] = (slot == narrow[:, k : k + 1].astype(jnp.int32)).astype(F32).astype(BF16)
        for u in late:
            ret[unit_at(*units[u][:2]), :] = jnp.zeros((count, dq), BF16)
        loads[2].wait()
        pltpu.make_async_copy(heads_in, heads_in, w_sem.at[3]).wait()
        here_cos = tab[pl.ds(2 * rows + e, 1), :]
        here_sin = tab[pl.ds(2 * rows + ep + e, 1), :]
        sign = jnp.where(lax.broadcasted_iota(jnp.int32, (BLOCK, hd), 1) < hd // 2, -1.0, 1.0)
        for b in range(blocks):
            at = slice(b * BLOCK, (b + 1) * BLOCK)
            cos, sin = tab[at, :], tab[slice(rows + b * BLOCK, rows + (b + 1) * BLOCK), :]
            turn[0, at, :] = cos * here_cos - sin * here_sin
            turn[1, at, :] = (sin * here_cos + cos * here_sin) * sign
            cums[at, :] = lax.dot_general(
                lower, narrow[at, :], (((1,), (0,)), ((), ())),
                preferred_element_type=F32, precision=lax.Precision.HIGHEST,
            )
        for n in range(heads):
            cols = slice(n * hd, (n + 1) * hd)
            total = None
            gone = None
            for b in range(blocks):
                at = slice(b * BLOCK, (b + 1) * BLOCK)
                cos, sin = turn[0, at, :], turn[1, at, :]

                def turned(ref):
                    val = ref[at, cols].astype(F32)
                    return val * cos + pltpu.roll(val, hd // 2, 1) * sin

                qb = turned(q_ref).astype(BF16)
                kb = (turned(k_ref) * factor).astype(BF16)
                vb = v_ref[at, cols]
                rq[at, cols] = qb
                cum = jnp.broadcast_to(cums[at, 4 + n : 5 + n], (BLOCK, BLOCK))
                spread = cum - cum.T
                weight = jnp.where(causal, jnp.exp(jnp.where(causal, spread, 0.0)), 0.0)
                scores = dot(qb, kb, ((1,), (1,)))
                inside[at, cols] = dot((scores * weight).astype(BF16), vb)
                ending = cum[BLOCK - 1 : BLOCK, :]
                k_hi, k_lo = split(kb.astype(F32) * jnp.exp(ending - cum))
                update = dot(k_hi, vb, ((0,), (0,))) + dot(k_lo, vb, ((0,), (0,)))
                if b == 0:
                    total, gone = update, ending
                else:
                    total = jnp.exp(ending) * total + update
                    gone = gone + ending
                if b < blocks - 1:
                    excl[1 + b, n * hd : (n + 1) * hd, :] = total
            state[0, n * hd : (n + 1) * hd, :] = total
            state[0, decay_at + n : decay_at + n + 1, :] = jnp.exp(gone)
        excl[0, :decay_at, :] = jnp.zeros((decay_at, hd), F32)

    def up_copy():
        return pltpu.make_async_remote_copy(
            src_ref=state.at[0], dst_ref=landed.at[0], send_sem=s_send.at[0],
            recv_sem=s_recv.at[0], device_id={"ep": e ^ 1}, device_id_type=MESH,
        )

    def next_copy():
        return pltpu.make_async_remote_copy(
            src_ref=passed.at[0], dst_ref=passed.at[1],
            send_sem=s_send.at[1], recv_sem=s_recv.at[1],
            device_id={"ep": lax.rem(e + 2, ep)}, device_id_type=MESH,
        )

    def down_copy():
        return pltpu.make_async_remote_copy(
            src_ref=passed.at[1], dst_ref=passed.at[1], send_sem=s_send.at[2], recv_sem=s_recv.at[2],
            device_id={"ep": e ^ 1}, device_id_type=MESH,
        )

    def decays(n):
        at = slice(decay_at + n, decay_at + n + 1)
        return landed[0, at, :], state[0, at, :]

    def scan_open():
        @pl.when(core == 1)
        def _():
            up_copy().wait_recv()
            for n in range(heads):
                at = slice(n * hd, (n + 1) * hd)
                mine = decays(n)[1]
                state[1, at, :] = mine * landed[0, at, :] + state[0, at, :]
                excl[0, at, :] = landed[0, at, :]
            passed[0] = state[1, :decay_at, :].astype(BF16)

        if chips > 1:

            @pl.when((core == 1) & (chip == 0))
            def _():
                next_copy().start()

    def scan_pass(turn_of):
        @pl.when((core == 1) & turn_of)
        def _():
            next_copy().wait_recv()
            down_copy().start()
            for n in range(heads):
                at = slice(n * hd, (n + 1) * hd)
                first, mine = decays(n)
                came = passed[1, at, :].astype(F32)
                passed[0, at, :] = ((first * mine) * came + state[1, at, :]).astype(BF16)
                excl[0, at, :] = first * came + excl[0, at, :]

        @pl.when((core == 1) & turn_of & (chip < chips - 1))
        def _():
            next_copy().start()

    def scan_close():
        @pl.when((core == 0) & (chip > 0))
        def _():
            down_copy().wait_recv()
            excl[0, :decay_at, :] = passed[1].astype(F32)

    def retention_close():
        for n in range(heads):
            cols = slice(n * hd, (n + 1) * hd)
            sat = slice(n * hd, (n + 1) * hd)
            entering = excl[0, sat, :]
            gone = None
            for b in range(blocks):
                at = slice(b * BLOCK, (b + 1) * BLOCK)
                cum = jnp.broadcast_to(cums[at, 4 + n : 5 + n], (BLOCK, hd))
                held = entering if b == 0 else jnp.exp(gone) * entering + excl[b, sat, :]
                hi, lo = split(held)
                qb = rq[at, cols]
                retained = inside[at, cols] + (dot(qb, hi) + dot(qb, lo)) * jnp.exp(cum)
                scale = lax.rsqrt(jnp.mean(retained * retained, axis=-1, keepdims=True) + 1e-05)
                gate = g_ref[at, cols].astype(F32)
                out = (retained * scale * (gate / (1.0 + jnp.exp(-gate)))).astype(BF16)
                ho[at, pl.ds(pl.multiple_of(t * heads * hd + n * hd, hd), hd)] = out
                ending = cum[BLOCK - 1 : BLOCK, :]
                gone = ending if gone is None else gone + ending

    for load in weight_loads[0]:
        load.wait()

    def take_partner(u):
        if units[u][0] <= 1 < units[u][0] + units[u][1]:
            z_copy(1, True, True).wait_recv()
        rows_start(u)
        rows_forward(u)
        rows_finish(u)

    def hidden(u):
        for j in range(len(first if u in (0, 4) else cuts)):
            hidden_piece(u, j)

    def forwards(u):
        for j in range(len(first if u in (0, 4) else cuts)):
            forward(u, j)

    take_partner(0)
    for j in range(len(first) - pieces + 1):
        hidden_piece(0, j)
    for j in range(1, pieces):
        for load in weight_loads[j]:
            load.wait()
        hidden_piece(0, j + len(first) - pieces)
    take_partner(1)
    hidden_piece(1, 0)
    retention_local()

    @pl.when(core == 0)
    def _():
        up_copy().start()

    for j in range(len(first) - 1):
        forward(0, j)
    for low, size, whole in units[5:]:
        group(low, size, 0, d)


    early = jnp.logical_not(inner) & (core == 0)

    @pl.when(early)
    def _():
        z_start(5)

    forward(0, len(first) - 1)
    rows_start(2)
    for j in range(1, pieces):
        hidden_piece(1, j)
    scan_open()

    rows_start(3)

    @pl.when(jnp.logical_not(early))
    def _():
        z_start(5)

    @pl.when(core == 0)
    def _():
        z_start(6)

    forward(1, 0)
    rows_forward(2)
    for j in range(1, pieces):
        forward(1, j)
    z_wait(4)
    hidden(4)
    scan_pass(chip == 1)

    @pl.when(core == 1)
    def _():
        z_start(6)

    rows_forward(3)
    rows_finish(2)
    hidden(2)
    forwards(4)
    rows_finish(3)
    hidden(3)

    @pl.when(core == 0)
    def _():
        z_start(7)

    loads[0].wait()
    down(0)
    forwards(2)

    def close():
        scan_close()
        retention_close()
        mix_gather(0).start()

    @pl.when(chip < 2)
    def _():
        close()

    z_wait(5)
    for j in range(pieces):
        hidden_piece(5, j)
        forward(3, j)
    scan_pass(chip == 2)

    @pl.when(core == 1)
    def _():
        z_start(7)

    down(1)
    ends = chip == chips - 1

    @pl.when(ends)
    def _():
        z_wait(6)
        hidden(6)

    scan_pass(chip > 2)

    @pl.when(chip >= 2)
    def _():
        close()

    down(4)

    @pl.when(jnp.logical_not(ends))
    def _():
        z_wait(6)
        hidden(6)

    forwards(5)
    down(2)
    z_wait(7)
    hidden(7)
    down(3)
    forwards(6)
    down_early(6)
    down(5)
    mix_gather(1).start()
    forwards(7)
    mix_gather(0).forward()
    down_early(7)
    down(6, True)
    loads[1].wait()
    mix_early(0)
    mix_gather(1).forward()
    mix_early(1)

    def taken(ref, sem):
        return pltpu.make_async_copy(ref, ref, sem)

    def weighed(first_pick, second_pick, came):
        return (
            dot(first_pick[...], came) * narrow[:, 2:3]
            + dot(second_pick[...], came) * narrow[:, 3:4]
        )

    taken(ret.at[: (ep - 1) * cap - ret_late.shape[0], :], r_recv.at[0]).wait()

    @pl.loop(0, dq // out_tile)
    def _(i):
        cols = pl.ds(pl.multiple_of(i * out_tile, out_tile), out_tile)
        combined[:, cols] = weighed(p0, p1, ret[:, cols])

    down(7, True)
    mix_project(0)
    mix_project(1)
    taken(ret_late, r_recv.at[1]).wait()

    @pl.loop(0, dq // out_tile)
    def _(i):
        cols = pl.ds(pl.multiple_of(i * out_tile, out_tile), out_tile)
        out_ref[1, :, cols] = (
            combined[:, cols] + weighed(late0, late1, ret_late[:, cols])
        ).astype(BF16)

    slim_rows = sum(offsets(u)[1] - offsets(u)[0] for u in range(4)) * cap
    taken(og.at[: ep * cap - cap - slim_rows, :], sent.at[0]).wait()
    taken(og.at[:slim_rows, :dq], sent.at[1]).wait()
    taken(x.at[:slim_rows, : (tp - 1) * dq], sent.at[2]).wait()
    taken(h.at[:, : (tp - 1) * fq], sent.at[3]).wait()
    taken(ho.at[:, : (tp - 1) * heads * hd], sent.at[4]).wait()
    taken(eo.at[: (ep - 1) * cap, :], sent.at[5]).wait()

    @pl.when(core == 0)
    def _():
        up_copy().wait_send()

    @pl.when((core == 1) & (chip < chips - 1))
    def _():
        next_copy().wait_send()

    @pl.when((core == 1) & (chip > 0))
    def _():
        down_copy().wait_send()


def turn_table(ep, rows, hd):
    half = hd // 2
    inverse = np.tile(10000.0 ** (-np.arange(half) / half), 2)
    near = np.arange(rows)[:, None] * inverse[None, :]
    far = (np.arange(ep) * rows)[:, None] * inverse[None, :]
    parts = [np.cos(near), np.sin(near), np.cos(far), np.sin(far)]
    return np.concatenate(parts).astype(np.float32)


def on_device(
    ep, tp,
    queries, keys, values, gates, log_decay, out_weight, moe_rows, moe_gain, routes,
    route_weights, gate_proj, up_proj, down_proj,
):
    rows, d = moe_rows.shape
    heads = log_decay.shape[1]
    width = queries.shape[1]
    hd = width // heads
    cap = 2 * rows // ep
    dq = d // tp
    fq = gate_proj.shape[2]
    ff = down_proj.shape[1]
    slots = 2 if tp == 4 else tp - 1
    units = plan(ep)
    slim = sum(size for low, size, whole in units if not whole) - 2
    blocks = rows // BLOCK
    srows = heads * hd + 8 * ((heads + 7) // 8)
    vmem = pl.BlockSpec(memory_space=pltpu.VMEM)
    dma = pltpu.SemaphoreType.DMA
    table = jnp.asarray(turn_table(ep, rows, hd))
    operands = [
        pltpu.with_memory_space_constraint(operand, pltpu.HBM)
        for operand in (
            queries, keys, values, gates, log_decay.T, table, moe_rows, moe_gain.reshape(-1, 128),
            routes.T, route_weights.T, out_weight, gate_proj, up_proj, down_proj,
        )
    ]
    both = pl.pallas_call(
        functools.partial(kernel, ep, tp),
        out_shape=jax.ShapeDtypeStruct((2, rows, dq), BF16),
        in_specs=[pl.BlockSpec(memory_space=pltpu.HBM)] * 14,
        out_specs=vmem,
        scratch_shapes=[
            pltpu.VMEM((heads, rows), F32),
            pltpu.VMEM((d // 128, 128), BF16),
            pltpu.VMEM((2, rows), jnp.int32),
            pltpu.VMEM((2, rows), F32),
            pltpu.VMEM((4, rows, width), BF16),
            pltpu.VMEM(table.shape, F32),
            pltpu.VMEM((rows, d), BF16),
            pltpu.VMEM((2, rows, hd), F32),
            pltpu.VMEM(out_weight.shape, BF16),
            pltpu.VMEM((d, fq), BF16),
            pltpu.VMEM((d, fq), BF16),
            pltpu.VMEM((ff, dq), BF16),
            pltpu.VMEM((rows, d), BF16),
            pltpu.VMEM((rows, ep * cap), BF16),
            pltpu.VMEM((rows, ep * cap), BF16),
            pltpu.VMEM((rows, ep // 4 * cap), BF16),
            pltpu.VMEM((rows, ep // 4 * cap), BF16),
            pltpu.VMEM((ep * cap, d), BF16),
            pltpu.VMEM((ep * cap, d), BF16),
            pltpu.VMEM((ep * cap, ff), BF16),
            pltpu.VMEM((ep * cap, dq), BF16),
            pltpu.VMEM((ep * cap, dq), BF16),
            pltpu.VMEM((ep // 4 * cap, dq), BF16),
            pltpu.VMEM((rows, dq), F32),
            pltpu.VMEM((rows, width * tp), BF16),
            pltpu.VMEM((2, srows, hd), F32),
            pltpu.VMEM((1, srows, hd), F32),
            pltpu.VMEM((2, heads * hd, hd), BF16),
            pltpu.VMEM((blocks, srows, hd), F32),
            pltpu.VMEM((2, ep // 8 * cap, dq), F32),
            pltpu.VMEM((rows, dq), F32),
            pltpu.VMEM((rows, width), BF16),
            pltpu.VMEM((rows, width), F32),
            pltpu.VMEM((rows, 128), F32),
            pltpu.VMEM((128, rows), F32),
            pltpu.VMEM((rows, 128), F32),
            dma((14,)), dma((6,)), dma((ep,)),
            dma((slim, slots)), dma((slim,)),
            dma((len(units) * 2 + 2, slots)), dma((len(units),)),
            dma((2,)),
            dma((2, slots)), dma((2,)),
            dma((3,)), dma((3,)),
        ],
        compiler_params=pltpu.CompilerParams(
            collective_id=0, has_side_effects=True, vmem_limit_bytes=44 * 1024 * 1024
        ),
    )(*operands)
    return both[0], both[1]


def solution(mesh):
    placed = (
        P("ep", "tp"), P("ep", "tp"), P("ep", "tp"), P("ep", "tp"), P("ep", "tp"),
        P(None, "tp"), P("ep", None), P(), P("ep", None), P("ep", None),
        P("ep", None, "tp"), P("ep", None, "tp"), P("ep", None, "tp"),
    )
    return jax.shard_map(
        functools.partial(on_device, mesh.shape["ep"], mesh.shape["tp"]),
        mesh=mesh, in_specs=placed, out_specs=(P("ep", "tp"), P("ep", "tp")), check_vma=False,
    )
```

```python
import functools

import jax
import jax.numpy as jnp
import numpy as np
from jax import lax
from jax.experimental import pallas as pl
from jax.experimental.pallas import tpu as pltpu
from jax.sharding import PartitionSpec as P

BLOCK = 128
MESH = pl.DeviceIdType.MESH
F32 = jnp.float32
BF16 = jnp.bfloat16


def each(low, high, body):
    if high - low <= 8:
        for index in range(low, high):
            body(index)
    else:

        @pl.loop(low, high)
        def _(index):
            body(index)


def span(index, size):
    return pl.ds(pl.multiple_of(index * size, size), size)


def split(value):
    high = value.astype(BF16)
    return high, (value - high.astype(F32)).astype(BF16)


def dot(a, b, dims=((1,), (0,))):
    return lax.dot_general(a, b, (dims, ((), ())), preferred_element_type=F32)


def plan(ep):
    q = ep // 8
    order = ((0, False), (1, False), (4, False), (6, False), (2, True), (5, True), (7, True), (3, True))
    return [(low * q, q, whole) for low, whole in order]


class Gather:
    def __init__(self, tp, region, half, send, recv, hop):
        self.tp, self.region, self.half, self.send = tp, region, half, send
        self.recv, self.hop = recv, hop
        self.me = lax.axis_index("tp")

    def copy(self, ref, recv, to):
        return pltpu.make_async_remote_copy(
            src_ref=ref, dst_ref=ref, send_sem=self.send, recv_sem=recv,
            device_id={"tp": to}, device_id_type=MESH,
        )

    def start(self):
        me, tp = self.me, self.tp
        if tp == 4:
            for k in (1, 2):
                self.copy(self.region(me), self.recv(k - 1), me ^ k).start()
        else:
            for k in range(1, tp):
                self.copy(self.region(me), self.recv(k - 1), lax.rem(me + k, tp)).start()

    def forward(self):
        if self.tp == 4:
            me = self.me
            for k in (1, 2):
                self.copy(self.region(me ^ k), self.recv(k - 1), me ^ k).wait_recv()
                self.copy(self.half(me ^ k, k - 1), self.hop, me ^ (3 - k)).start()

    def finish(self):
        me, tp = self.me, self.tp
        if tp == 4:
            self.copy(self.region(me ^ 3), self.hop, me ^ 3).wait_recv()
        else:
            for k in range(1, tp):
                owner = lax.rem(me + tp - k, tp)
                self.copy(self.region(owner), self.recv(k - 1), owner).wait_recv()


def kernel(
    ep, tp,
    q_hbm, k_hbm, v_hbm, g_hbm, ld_hbm, tab_hbm, rows_hbm, gain_hbm, routes_hbm, rw_hbm,
    wo_hbm, wg_hbm, wu_hbm, wd_hbm,
    out_ref,
    ld_ref, gain_ref, routes_ref, rw_ref, heads_in, tab, rows_ref, turn,
    wo, wg, wu, wd, normed, p0, p1, late0, late1, og, x, h, eo, ret, ret_late, combined, ho, state, landed, passed, excl, partial, mixed,
    rq, inside, cums, pack, narrow,
    w_sem, sent, z_recv, f_recv, f_hop, h_recv, h_hop, r_recv, m_recv, m_hop, s_send, s_recv,
):

    e, t = lax.axis_index("ep"), lax.axis_index("tp")
    rows, d = rows_ref.shape
    cap = 2 * rows // ep
    dq = d // tp
    ff = wd.shape[0]
    fq = ff // tp
    heads = ld_ref.shape[0]
    hd = heads_in.shape[2] // heads
    q_ref, k_ref, v_ref, g_ref = [heads_in.at[i] for i in range(4)]
    blocks = rows // BLOCK
    g = ep // 4
    units = plan(ep)
    tile = min(256, fq)
    pieces = 2 if fq >= 512 else 1
    piece = fq // pieces
    cuts = [(j * piece, piece) for j in range(pieces)]
    first = [(0, tile), (tile, piece - tile)] * (piece > tile) + cuts[piece > tile :]
    core, chip, chips = lax.rem(e, 2), e // 2, ep // 2
    inner = lax.rem(chip + chip // 2, 2) == 1

    barrier = pltpu.get_barrier_semaphore()

    def greet_ep(off):
        pl.semaphore_signal(barrier, inc=1, device_id={"ep": e ^ off}, device_id_type=MESH)

    each(1, ep, greet_ep)
    for k in range(1, tp):
        pl.semaphore_signal(
            barrier, inc=1, device_id={"tp": lax.rem(t + k, tp)}, device_id_type=MESH
        )

    parts = 2
    step_rows = rows // parts
    part_at = [slice(i * step_rows, (i + 1) * step_rows) for i in range(parts)]
    row_loads = [
        pltpu.make_async_copy(rows_hbm.at[at, :], rows_ref.at[at, :], w_sem.at[4 + i])
        for i, at in enumerate(part_at)
    ]
    loads = [
        pltpu.make_async_copy(src, dst, w_sem.at[i])
        for i, (src, dst) in enumerate(
            (
                (wd_hbm.at[0], wd), (wo_hbm, wo), (tab_hbm, tab),
            )
        )
    ]
    head_loads = [
        pltpu.make_async_copy(src, dst, w_sem.at[3])
        for src, dst in ((q_hbm, q_ref), (k_hbm, k_ref), (v_hbm, v_ref), (g_hbm, g_ref))
    ]
    weight_loads = [
        [
            pltpu.make_async_copy(
                src.at[0, :, j * piece : (j + 1) * piece], dst.at[:, j * piece : (j + 1) * piece],
                w_sem.at[6 + 2 * j + i],
            )
            for i, (src, dst) in enumerate(((wg_hbm, wg), (wu_hbm, wu)))
        ]
        for j in range(pieces)
    ]
    small_loads = [
        pltpu.make_async_copy(src, dst, w_sem.at[10 + i])
        for i, (src, dst) in enumerate(
            (
                (routes_hbm, routes_ref), (gain_hbm, gain_ref), (ld_hbm, ld_ref), (rw_hbm, rw_ref),
            )
        )
    ]
    for load in row_loads + small_loads + sum(weight_loads, []):
        load.start()

    small_loads[0].wait()
    routes = [routes_ref[k : k + 1, :] for k in range(2)]
    experts = lax.broadcasted_iota(jnp.int32, (max(8, ep), rows), 0)
    hot = [(experts == routes[k]).astype(F32) for k in range(2)]
    before = (
        lax.broadcasted_iota(jnp.int32, (rows, rows), 0)
        < lax.broadcasted_iota(jnp.int32, (rows, rows), 1)
    ).astype(F32).astype(BF16)
    rank = dot((hot[0] + hot[1]).astype(BF16), before)
    targets = [
        routes[k] * cap + jnp.sum(rank * hot[k], axis=0, keepdims=True).astype(jnp.int32)
        for k in range(2)
    ]

    small_loads[1].wait()
    for i, at in enumerate(part_at):
        row_loads[i].wait()
        squares = None
        for c in range(d // 128):
            val = rows_ref[at, c * 128 : (c + 1) * 128].astype(F32)
            squares = val * val if squares is None else squares + val * val
        scale = lax.rsqrt(jnp.sum(squares, axis=-1, keepdims=True) / d + 1e-06)
        for c in range(d // 128):
            cols = slice(c * 128, (c + 1) * 128)
            val = rows_ref[at, cols].astype(F32)
            normed[at, cols] = (val * scale * gain_ref[c : c + 1, :].astype(F32)).astype(BF16)

    late = (6, 7)

    def group_of(low, size):
        return (e // size) ^ (low // size)

    def unit_at(low, size):
        return span(group_of(low, size), size * cap)

    def pick(low, size):
        slot = lax.broadcasted_iota(jnp.int32, (size * cap, rows), 0) + (
            (e // size) ^ (low // size)
        ) * (size * cap)
        return ((slot == targets[0]) | (slot == targets[1])).astype(F32).astype(BF16)

    def group(low, size, start, width):
        chosen = pick(low, size)
        wide = min(256, width)
        for c in range(width // wide):
            cols = pl.ds(pl.multiple_of(start + c * wide, wide), wide)
            og[unit_at(low, size), cols] = dot(chosen, normed[:, cols]).astype(BF16)

    group(0, g, 0, d)
    for low, size, whole in units[2:4]:
        group(low, size, t * dq, dq)
    pl.semaphore_wait(barrier, ep - 1 + tp - 1)

    def z_copy(off, here, whole):
        other = e ^ off
        land = span(other if here else e, cap)
        if whole:
            src, dst = og.at[span(other, cap), :], x.at[land, :]
        else:
            src, dst = og.at[span(other, cap), span(t, dq)], x.at[land, span(t, dq)]
        return pltpu.make_async_remote_copy(
            src_ref=src, dst_ref=dst, send_sem=sent.at[0 if whole else 1],
            recv_sem=z_recv.at[other if here else e],
            device_id={"ep": other}, device_id_type=MESH,
        )

    def offsets(u):
        low, size, whole = units[u]
        return max(2, low), max(2, low + size), whole

    def z_start(u):
        low, high, whole = offsets(u)
        each(low, high, lambda off: z_copy(off, False, whole).start())

    def z_wait(u):
        low, high, whole = offsets(u)
        each(low, high, lambda off: z_copy(off, True, whole).wait_recv())

    z_copy(1, False, True).start()
    for u in range(4):
        z_start(u)
    for load in head_loads + loads[2:3] + loads[0:2]:
        load.start()
    x[span(e, cap), :] = og[span(e, cap), :]
    group(*units[4][:2], 0, d)
    z_start(4)

    slim_at, count = [], 0
    for u in range(4):
        low, high, _ = offsets(u)
        slim_at.append(count - low)
        count += high - low

    def row_gather(u, off):
        other = e ^ off
        start = other * cap
        at = slim_at[u] + off

        def half(owner, k):
            return x.at[
                pl.ds(pl.multiple_of(start + k * (cap // 2), cap // 2), cap // 2), span(owner, dq)
            ]

        return Gather(
            tp, lambda owner: x.at[span(other, cap), span(owner, dq)], half,
            sent.at[2], lambda slot: f_recv.at[at, slot], f_hop.at[at],
        )

    def rows_start(u):
        low, high, _ = offsets(u)

        def take(off):
            z_copy(off, True, False).wait_recv()
            row_gather(u, off).start()

        each(low, high, take)

    def rows_forward(u):
        low, high, _ = offsets(u)
        each(low, high, lambda off: row_gather(u, off).forward())

    def rows_finish(u):
        low, high, _ = offsets(u)
        each(low, high, lambda off: row_gather(u, off).finish())

    counts = [len(first if u in (0, 4, 5) else cuts) for u in range(len(units))]
    piece_at = [sum(counts[:u]) for u in range(len(units))]

    def hid_gather(u, number):
        start, width = (0, fq) if number is None else (first if u in (0, 4, 5) else cuts)[number]
        low, size, _ = units[u]
        count = size * cap
        base = ((e // size) ^ (low // size)) * count

        def cols(owner):
            return pl.ds(pl.multiple_of(owner * fq + start, tile), width)

        return Gather(
            tp,
            lambda owner: h.at[pl.ds(pl.multiple_of(base, count), count), cols(owner)],
            lambda owner, k: h.at[
                pl.ds(pl.multiple_of(base + k * (count // 2), count // 2), count // 2), cols(owner)
            ],
            sent.at[3], lambda slot: h_recv.at[piece_at[u] + number, slot], h_hop.at[u],
        )

    def hid_finish(u):
        if tp == 4:
            hid_gather(u, None).finish()
        else:
            for j in range(len(first if u in (0, 4, 5) else cuts)):
                hid_gather(u, j).finish()

    half_rows = rows // 2

    def mix_gather(b):
        def at(low, size):
            return slice(b * half_rows + low, b * half_rows + low + size)

        return Gather(
            tp, lambda owner: ho.at[at(0, half_rows), span(owner, heads * hd)],
            lambda owner, k: ho.at[
                at(k * (half_rows // 2), half_rows // 2), span(owner, heads * hd)
            ],
            sent.at[4], lambda slot: m_recv.at[b, slot], m_hop.at[b],
        )

    def hidden_piece(u, j):
        at = unit_at(*units[u][:2])
        start, width = (first if u in (0, 4, 5) else cuts)[j]

        @pl.loop(0, width // tile)
        def _(i):
            cols = pl.ds(pl.multiple_of(start + i * tile, tile), tile)
            held = x[at, :]
            gate = dot(held, wg[:, cols])
            up = dot(held, wu[:, cols])
            hid = (gate / (1.0 + jnp.exp(-gate)) * up).astype(BF16)
            h[at, pl.ds(pl.multiple_of(t * fq + start + i * tile, tile), tile)] = hid

        hid_gather(u, j).start()

    def back_copy(u, off, cols):
        other = e ^ off
        size = units[u][1]
        if u in late:
            row = late.index(u) * size + lax.rem(e, size)
            dst = ret_late.at[pl.ds(pl.multiple_of(row * cap, cap), cap), cols]
        else:
            dst = ret.at[span(e, cap), cols]
        return pltpu.make_async_remote_copy(
            src_ref=eo.at[span(other, cap), cols], dst_ref=dst,
            send_sem=sent.at[5], recv_sem=r_recv.at[1 if u in late else 0],
            device_id={"ep": other}, device_id_type=MESH,
        )

    out_tile = min(256, dq)

    def mix_early(b):
        if tp == 4:
            at = slice(b * half_rows, (b + 1) * half_rows)
            share = heads * hd

            @pl.loop(0, dq // out_tile)
            def _(i):
                cols = pl.ds(pl.multiple_of(i * out_tile, out_tile), out_tile)
                mixed[at, cols] = sum(
                    dot(ho[at, span(t ^ k, share)], wo[span(t ^ k, share), cols]) for k in range(3)
                )

    def mix_project(b):
        mix_gather(b).finish()
        at = slice(b * half_rows, (b + 1) * half_rows)
        share = heads * hd

        @pl.loop(0, dq // out_tile)
        def _(i):
            cols = pl.ds(pl.multiple_of(i * out_tile, out_tile), out_tile)
            if tp == 4:
                total = mixed[at, cols] + dot(
                    ho[at, span(t ^ 3, share)], wo[span(t ^ 3, share), cols]
                )
            else:
                total = dot(ho[at, :], wo[:, cols])
            out_ref[0, at, cols] = total.astype(BF16)

    def down_early(u):
        if tp == 4:
            at = unit_at(*units[u][:2])

            @pl.loop(0, dq // out_tile)
            def _(i):
                cols = pl.ds(pl.multiple_of(i * out_tile, out_tile), out_tile)
                partial[u % 2, :, cols] = sum(
                    dot(h[at, span(t ^ k, fq)], wd[span(t ^ k, fq), cols]) for k in range(3)
                )

    def down(u, early=False):
        hid_finish(u)
        low, size, _ = units[u]
        at = unit_at(low, size)

        @pl.loop(0, dq // out_tile)
        def _(i):
            cols = pl.ds(pl.multiple_of(i * out_tile, out_tile), out_tile)
            if early and tp == 4:
                done = t ^ 3
                total = partial[u % 2, :, cols] + dot(
                    h[at, span(done, fq)], wd[span(done, fq), cols]
                )
            else:
                total = dot(h[at, :], wd[:, cols])
            eo[at, cols] = total.astype(BF16)
            each(max(1, low), low + size, lambda off: back_copy(u, off, cols).start())

        if low == 0:
            ret[span(e, cap), :] = eo[span(e, cap), :]

    def forward(u, j):
        hid_gather(u, j).forward()

    row_i = lax.broadcasted_iota(jnp.int32, (BLOCK, BLOCK), 0)
    col_j = lax.broadcasted_iota(jnp.int32, (BLOCK, BLOCK), 1)
    causal = row_i >= col_j
    lower = causal.astype(F32)
    factor = hd ** (-0.5)
    decay_at = heads * hd

    def retention_local():
        small_loads[2].wait()
        small_loads[3].wait()
        pack[...] = jnp.zeros_like(pack)
        pack[0:1, :] = targets[0].astype(F32)
        pack[1:2, :] = targets[1].astype(F32)
        pack[2:4, :] = rw_ref[...]
        pack[4 : 4 + heads, :] = ld_ref[...]
        for b in range(rows // 128):
            narrow[b * 128 : (b + 1) * 128, :] = pack[:, b * 128 : (b + 1) * 128].T
        lanes = lax.broadcasted_iota(jnp.int32, (rows, ep * cap), 1)
        for k, ref in ((0, p0), (1, p1)):
            ref[...] = (lanes == narrow[:, k : k + 1].astype(jnp.int32)).astype(F32).astype(BF16)
        count = units[late[0]][1] * cap
        place = lax.broadcasted_iota(jnp.int32, (rows, 2 * count), 1)
        bases = [group_of(*units[u][:2]) * count for u in late]
        slot = jnp.where(place < count, place + bases[0], place - count + bases[1])
        for k, ref in ((0, late0), (1, late1)):
            ref[...] = (slot == narrow[:, k : k + 1].astype(jnp.int32)).astype(F32).astype(BF16)
        for u in late:
            ret[unit_at(*units[u][:2]), :] = jnp.zeros((count, dq), BF16)
        loads[2].wait()
        pltpu.make_async_copy(heads_in, heads_in, w_sem.at[3]).wait()
        here_cos = tab[pl.ds(2 * rows + e, 1), :]
        here_sin = tab[pl.ds(2 * rows + ep + e, 1), :]
        sign = jnp.where(lax.broadcasted_iota(jnp.int32, (BLOCK, hd), 1) < hd // 2, -1.0, 1.0)
        for b in range(blocks):
            at = slice(b * BLOCK, (b + 1) * BLOCK)
            cos, sin = tab[at, :], tab[slice(rows + b * BLOCK, rows + (b + 1) * BLOCK), :]
            turn[0, at, :] = cos * here_cos - sin * here_sin
            turn[1, at, :] = (sin * here_cos + cos * here_sin) * sign
            cums[at, :] = lax.dot_general(
                lower, narrow[at, :], (((1,), (0,)), ((), ())),
                preferred_element_type=F32, precision=lax.Precision.HIGHEST,
            )
        for n in range(heads):
            cols = slice(n * hd, (n + 1) * hd)
            total = None
            gone = None
            for b in range(blocks):
                at = slice(b * BLOCK, (b + 1) * BLOCK)
                cos, sin = turn[0, at, :], turn[1, at, :]

                def turned(ref):
                    val = ref[at, cols].astype(F32)
                    return val * cos + pltpu.roll(val, hd // 2, 1) * sin

                qb = turned(q_ref).astype(BF16)
                kb = (turned(k_ref) * factor).astype(BF16)
                vb = v_ref[at, cols]
                rq[at, cols] = qb
                cum = jnp.broadcast_to(cums[at, 4 + n : 5 + n], (BLOCK, BLOCK))
                spread = cum - cum.T
                weight = jnp.where(causal, jnp.exp(jnp.where(causal, spread, 0.0)), 0.0)
                scores = dot(qb, kb, ((1,), (1,)))
                inside[at, cols] = dot((scores * weight).astype(BF16), vb)
                ending = cum[BLOCK - 1 : BLOCK, :]
                k_hi, k_lo = split(kb.astype(F32) * jnp.exp(ending - cum))
                update = dot(k_hi, vb, ((0,), (0,))) + dot(k_lo, vb, ((0,), (0,)))
                if b == 0:
                    total, gone = update, ending
                else:
                    total = jnp.exp(ending) * total + update
                    gone = gone + ending
                if b < blocks - 1:
                    excl[1 + b, n * hd : (n + 1) * hd, :] = total
            state[0, n * hd : (n + 1) * hd, :] = total
            state[0, decay_at + n : decay_at + n + 1, :] = jnp.exp(gone)
        excl[0, :decay_at, :] = jnp.zeros((decay_at, hd), F32)

    def up_copy():
        return pltpu.make_async_remote_copy(
            src_ref=state.at[0], dst_ref=landed.at[0], send_sem=s_send.at[0],
            recv_sem=s_recv.at[0], device_id={"ep": e ^ 1}, device_id_type=MESH,
        )

    def next_copy():
        return pltpu.make_async_remote_copy(
            src_ref=passed.at[0], dst_ref=passed.at[1],
            send_sem=s_send.at[1], recv_sem=s_recv.at[1],
            device_id={"ep": lax.rem(e + 2, ep)}, device_id_type=MESH,
        )

    def down_copy():
        return pltpu.make_async_remote_copy(
            src_ref=passed.at[1], dst_ref=passed.at[1], send_sem=s_send.at[2], recv_sem=s_recv.at[2],
            device_id={"ep": e ^ 1}, device_id_type=MESH,
        )

    def decays(n):
        at = slice(decay_at + n, decay_at + n + 1)
        return landed[0, at, :], state[0, at, :]

    def scan_open():
        @pl.when(core == 1)
        def _():
            up_copy().wait_recv()
            for n in range(heads):
                at = slice(n * hd, (n + 1) * hd)
                mine = decays(n)[1]
                state[1, at, :] = mine * landed[0, at, :] + state[0, at, :]
                excl[0, at, :] = landed[0, at, :]
            passed[0] = state[1, :decay_at, :].astype(BF16)

        if chips > 1:

            @pl.when((core == 1) & (chip == 0))
            def _():
                next_copy().start()

    def scan_pass(turn_of):
        @pl.when((core == 1) & turn_of)
        def _():
            next_copy().wait_recv()
            down_copy().start()
            for n in range(heads):
                at = slice(n * hd, (n + 1) * hd)
                first, mine = decays(n)
                came = passed[1, at, :].astype(F32)
                passed[0, at, :] = ((first * mine) * came + state[1, at, :]).astype(BF16)
                excl[0, at, :] = first * came + excl[0, at, :]

        @pl.when((core == 1) & turn_of & (chip < chips - 1))
        def _():
            next_copy().start()

    def scan_close():
        @pl.when((core == 0) & (chip > 0))
        def _():
            down_copy().wait_recv()
            excl[0, :decay_at, :] = passed[1].astype(F32)

    def retention_close():
        for n in range(heads):
            cols = slice(n * hd, (n + 1) * hd)
            sat = slice(n * hd, (n + 1) * hd)
            entering = excl[0, sat, :]
            gone = None
            for b in range(blocks):
                at = slice(b * BLOCK, (b + 1) * BLOCK)
                cum = jnp.broadcast_to(cums[at, 4 + n : 5 + n], (BLOCK, hd))
                held = entering if b == 0 else jnp.exp(gone) * entering + excl[b, sat, :]
                hi, lo = split(held)
                qb = rq[at, cols]
                retained = inside[at, cols] + (dot(qb, hi) + dot(qb, lo)) * jnp.exp(cum)
                scale = lax.rsqrt(jnp.mean(retained * retained, axis=-1, keepdims=True) + 1e-05)
                gate = g_ref[at, cols].astype(F32)
                out = (retained * scale * (gate / (1.0 + jnp.exp(-gate)))).astype(BF16)
                ho[at, pl.ds(pl.multiple_of(t * heads * hd + n * hd, hd), hd)] = out
                ending = cum[BLOCK - 1 : BLOCK, :]
                gone = ending if gone is None else gone + ending

    for load in weight_loads[0]:
        load.wait()

    def take_partner(u):
        if units[u][0] <= 1 < units[u][0] + units[u][1]:
            z_copy(1, True, True).wait_recv()
        rows_start(u)
        rows_forward(u)
        rows_finish(u)

    def hidden(u):
        for j in range(len(first if u in (0, 4, 5) else cuts)):
            hidden_piece(u, j)

    def forwards(u):
        for j in range(len(first if u in (0, 4, 5) else cuts)):
            forward(u, j)

    take_partner(0)
    for j in range(len(first) - pieces + 1):
        hidden_piece(0, j)
    for j in range(1, pieces):
        for load in weight_loads[j]:
            load.wait()
        hidden_piece(0, j + len(first) - pieces)
    take_partner(1)
    hidden_piece(1, 0)
    retention_local()

    @pl.when(core == 0)
    def _():
        up_copy().start()

    for j in range(len(first) - 1):
        forward(0, j)
    for low, size, whole in units[5:]:
        group(low, size, 0, d)


    early = jnp.logical_not(inner) & (core == 0)

    @pl.when(early)
    def _():
        z_start(5)

    forward(0, len(first) - 1)
    rows_start(2)
    for j in range(1, pieces):
        hidden_piece(1, j)
    scan_open()

    rows_start(3)

    @pl.when(jnp.logical_not(early))
    def _():
        z_start(5)

    @pl.when(core == 0)
    def _():
        z_start(6)

    forward(1, 0)
    rows_forward(2)
    for j in range(1, pieces):
        forward(1, j)
    z_wait(4)
    hidden(4)
    scan_pass(chip == 1)

    @pl.when(core == 1)
    def _():
        z_start(6)

    rows_forward(3)
    rows_finish(2)
    hidden(2)
    forwards(4)
    rows_finish(3)
    hidden(3)

    @pl.when(core == 0)
    def _():
        z_start(7)

    loads[0].wait()
    down(0)
    forwards(2)

    def close():
        scan_close()
        retention_close()
        mix_gather(0).start()

    @pl.when(chip < 2)
    def _():
        close()

    z_wait(5)
    more = len(first) - pieces
    for j in range(more):
        hidden_piece(5, j)
    for j in range(pieces):
        hidden_piece(5, j + more)
        forward(3, j)
    scan_pass(chip == 2)

    @pl.when(core == 1)
    def _():
        z_start(7)

    down(1)
    ends = chip == chips - 1

    @pl.when(ends)
    def _():
        z_wait(6)
        hidden(6)

    scan_pass(chip > 2)

    @pl.when(chip >= 2)
    def _():
        close()

    down(4)

    @pl.when(jnp.logical_not(ends))
    def _():
        z_wait(6)
        hidden(6)

    forwards(5)
    down(2)
    z_wait(7)
    hidden(7)
    down(3)
    forwards(6)
    down_early(6)
    down(5)
    mix_gather(1).start()
    forwards(7)
    mix_gather(0).forward()
    down_early(7)
    down(6, True)
    loads[1].wait()
    mix_early(0)
    mix_gather(1).forward()
    mix_early(1)

    def taken(ref, sem):
        return pltpu.make_async_copy(ref, ref, sem)

    def weighed(first_pick, second_pick, came):
        return (
            dot(first_pick[...], came) * narrow[:, 2:3]
            + dot(second_pick[...], came) * narrow[:, 3:4]
        )

    taken(ret.at[: (ep - 1) * cap - ret_late.shape[0], :], r_recv.at[0]).wait()

    @pl.loop(0, dq // out_tile)
    def _(i):
        cols = pl.ds(pl.multiple_of(i * out_tile, out_tile), out_tile)
        combined[:, cols] = weighed(p0, p1, ret[:, cols])

    down(7, True)
    mix_project(0)
    mix_project(1)
    taken(ret_late, r_recv.at[1]).wait()

    @pl.loop(0, dq // out_tile)
    def _(i):
        cols = pl.ds(pl.multiple_of(i * out_tile, out_tile), out_tile)
        out_ref[1, :, cols] = (
            combined[:, cols] + weighed(late0, late1, ret_late[:, cols])
        ).astype(BF16)

    slim_rows = sum(offsets(u)[1] - offsets(u)[0] for u in range(4)) * cap
    taken(og.at[: ep * cap - cap - slim_rows, :], sent.at[0]).wait()
    taken(og.at[:slim_rows, :dq], sent.at[1]).wait()
    taken(x.at[:slim_rows, : (tp - 1) * dq], sent.at[2]).wait()
    taken(h.at[:, : (tp - 1) * fq], sent.at[3]).wait()
    taken(ho.at[:, : (tp - 1) * heads * hd], sent.at[4]).wait()
    taken(eo.at[: (ep - 1) * cap, :], sent.at[5]).wait()

    @pl.when(core == 0)
    def _():
        up_copy().wait_send()

    @pl.when((core == 1) & (chip < chips - 1))
    def _():
        next_copy().wait_send()

    @pl.when((core == 1) & (chip > 0))
    def _():
        down_copy().wait_send()


def turn_table(ep, rows, hd):
    half = hd // 2
    inverse = np.tile(10000.0 ** (-np.arange(half) / half), 2)
    near = np.arange(rows)[:, None] * inverse[None, :]
    far = (np.arange(ep) * rows)[:, None] * inverse[None, :]
    parts = [np.cos(near), np.sin(near), np.cos(far), np.sin(far)]
    return np.concatenate(parts).astype(np.float32)


def on_device(
    ep, tp,
    queries, keys, values, gates, log_decay, out_weight, moe_rows, moe_gain, routes,
    route_weights, gate_proj, up_proj, down_proj,
):
    rows, d = moe_rows.shape
    heads = log_decay.shape[1]
    width = queries.shape[1]
    hd = width // heads
    cap = 2 * rows // ep
    dq = d // tp
    fq = gate_proj.shape[2]
    ff = down_proj.shape[1]
    slots = 2 if tp == 4 else tp - 1
    units = plan(ep)
    slim = sum(size for low, size, whole in units if not whole) - 2
    blocks = rows // BLOCK
    srows = heads * hd + 8 * ((heads + 7) // 8)
    vmem = pl.BlockSpec(memory_space=pltpu.VMEM)
    dma = pltpu.SemaphoreType.DMA
    table = jnp.asarray(turn_table(ep, rows, hd))
    operands = [
        pltpu.with_memory_space_constraint(operand, pltpu.HBM)
        for operand in (
            queries, keys, values, gates, log_decay.T, table, moe_rows, moe_gain.reshape(-1, 128),
            routes.T, route_weights.T, out_weight, gate_proj, up_proj, down_proj,
        )
    ]
    both = pl.pallas_call(
        functools.partial(kernel, ep, tp),
        out_shape=jax.ShapeDtypeStruct((2, rows, dq), BF16),
        in_specs=[pl.BlockSpec(memory_space=pltpu.HBM)] * 14,
        out_specs=vmem,
        scratch_shapes=[
            pltpu.VMEM((heads, rows), F32),
            pltpu.VMEM((d // 128, 128), BF16),
            pltpu.VMEM((2, rows), jnp.int32),
            pltpu.VMEM((2, rows), F32),
            pltpu.VMEM((4, rows, width), BF16),
            pltpu.VMEM(table.shape, F32),
            pltpu.VMEM((rows, d), BF16),
            pltpu.VMEM((2, rows, hd), F32),
            pltpu.VMEM(out_weight.shape, BF16),
            pltpu.VMEM((d, fq), BF16),
            pltpu.VMEM((d, fq), BF16),
            pltpu.VMEM((ff, dq), BF16),
            pltpu.VMEM((rows, d), BF16),
            pltpu.VMEM((rows, ep * cap), BF16),
            pltpu.VMEM((rows, ep * cap), BF16),
            pltpu.VMEM((rows, ep // 4 * cap), BF16),
            pltpu.VMEM((rows, ep // 4 * cap), BF16),
            pltpu.VMEM((ep * cap, d), BF16),
            pltpu.VMEM((ep * cap, d), BF16),
            pltpu.VMEM((ep * cap, ff), BF16),
            pltpu.VMEM((ep * cap, dq), BF16),
            pltpu.VMEM((ep * cap, dq), BF16),
            pltpu.VMEM((ep // 4 * cap, dq), BF16),
            pltpu.VMEM((rows, dq), F32),
            pltpu.VMEM((rows, width * tp), BF16),
            pltpu.VMEM((2, srows, hd), F32),
            pltpu.VMEM((1, srows, hd), F32),
            pltpu.VMEM((2, heads * hd, hd), BF16),
            pltpu.VMEM((blocks, srows, hd), F32),
            pltpu.VMEM((2, ep // 8 * cap, dq), F32),
            pltpu.VMEM((rows, dq), F32),
            pltpu.VMEM((rows, width), BF16),
            pltpu.VMEM((rows, width), F32),
            pltpu.VMEM((rows, 128), F32),
            pltpu.VMEM((128, rows), F32),
            pltpu.VMEM((rows, 128), F32),
            dma((14,)), dma((6,)), dma((ep,)),
            dma((slim, slots)), dma((slim,)),
            dma((len(units) * 2 + 3, slots)), dma((len(units),)),
            dma((2,)),
            dma((2, slots)), dma((2,)),
            dma((3,)), dma((3,)),
        ],
        compiler_params=pltpu.CompilerParams(
            collective_id=0, has_side_effects=True, vmem_limit_bytes=44 * 1024 * 1024
        ),
    )(*operands)
    return both[0], both[1]


def solution(mesh):
    placed = (
        P("ep", "tp"), P("ep", "tp"), P("ep", "tp"), P("ep", "tp"), P("ep", "tp"),
        P(None, "tp"), P("ep", None), P(), P("ep", None), P("ep", None),
        P("ep", None, "tp"), P("ep", None, "tp"), P("ep", None, "tp"),
    )
    return jax.shard_map(
        functools.partial(on_device, mesh.shape["ep"], mesh.shape["tp"]),
        mesh=mesh, in_specs=placed, out_specs=(P("ep", "tp"), P("ep", "tp")), check_vma=False,
    )
```
